256 devices in a mesh: grp: 2 (over y), ep: 32 (over z, core), tp: 4 (over x).
Axes of the slice: x: 4, y: 2, z: 16, core: 2. Of those that a mesh axis runs over, the one named last changes fastest.
The devices are a block of a 4x16x16 slice.
Arguments:
- query_vectors: bfloat16 [32768, 2048], P(('grp', 'ep'), 'tp'), parts along dimension 0, may hold values from -6 to 6
- attend_lookup_vectors: bfloat16 [32768, 2048], P(('grp', 'ep'), 'tp'), parts along dimension 0, may hold values from -6 to 6
- attend_content_vectors: bfloat16 [32768, 2048], P(('grp', 'ep'), 'tp'), parts along dimension 0, may hold values from -6 to 6
- forget_speed_dependent: bfloat16 [32768, 2048], P(('grp', 'ep'), 'tp'), parts along dimension 0, may hold values from -3 to 3
- amend_speed_dependent: bfloat16 [32768, 2048], P(('grp', 'ep'), 'tp'), parts along dimension 0, may hold values from -6 to 6
- result_switch_preactivation: bfloat16 [32768, 2048], P(('grp', 'ep'), 'tp'), parts along dimension 0, may hold values from -6 to 6
- feature_forget_baseline: float32 [2048], P('tp'), may hold values from -13 to -3
- amend_speed_baseline: float32 [2048], P('tp'), may hold values from -9 to 3
- sudden_forget_extra: float32 [32768, 32], P(('grp', 'ep'), 'tp'), parts along dimension 0, may hold values from -1 to 0
- group_scaling_factor: float32 [2048], P('tp'), may hold values from 0.1 to 1.9
- result_mapping_matrix: bfloat16 [2048, 2048], P('tp'), may hold values from -0.125 to 0.125
- specialist_tokens_activations: bfloat16 [32768, 2048], P(('grp', 'ep', 'tp')), parts along dimension 0, may hold values from -6 to 6
- specialist_scaling_factor: float32 [2048], replicated, may hold values from 0.1 to 1.9
- selected_specialists: int32 [32768, 2], P(('grp', 'ep', 'tp')), parts along dimension 0, may hold values from 0 to 31, all different within a row; in each aligned block of 128 rows (0 to 127, 128 to 255, ...) at most 12 rows name the same one
- selection_mixing_factors: float32 [32768, 2], P(('grp', 'ep', 'tp')), parts along dimension 0, may hold values from 0.3 to 1.5
- dispatched_switch_matrix: bfloat16 [32, 2048, 1024], P('ep', None, 'tp'), may hold values from -0.125 to 0.125
- dispatched_raising_matrix: bfloat16 [32, 2048, 1024], P('ep', None, 'tp'), may hold values from -0.125 to 0.125
- dispatched_lowering_matrix: bfloat16 [32, 1024, 2048], P('ep', 'tp'), may hold values from -0.1875 to 0.1875
- common_switch_matrix: bfloat16 [2048, 512], P(None, 'tp'), may hold values from -0.125 to 0.125
- common_raising_matrix: bfloat16 [2048, 512], P(None, 'tp'), may hold values from -0.125 to 0.125
- common_lowering_matrix: bfloat16 [512, 2048], P('tp'), may hold values from -0.25 to 0.25
Outputs:
- attend_result_matrix: bfloat16 [32768, 2048], P(('grp', 'ep', 'tp')), parts along dimension 0
- moe_out: bfloat16 [32768, 2048], P(('grp', 'ep', 'tp')), parts along dimension 0
The draws below stay inside these ranges and needn't reach their ends.
There are 2 independent parts, one for each index of `grp`. The reference program is written for one: setup_inputs(seed, part) draws one part's arguments, and reference() takes and returns one part's arrays. A program takes and returns all parts, laid end to end along the dimension named above; an argument that names none is the same for every part. Nothing has to cross between parts.
Inputs may be any that keep to these rules, and one draw needn't show every extreme that they name: `selected_specialists`: each row names 2 different experts. Among the rows of one device no expert is named more than 12 times, and in every draw some device names some expert exactly 12 times.
All inputs are finite; a program needn't handle non-finite values.
Results may differ from the reference program's by a relative error of at most 0.023.
Values may be sent and summed in bfloat16 or wider, within the bound.
No kernel may reach another device: no remote copies, remote signals or barrier semaphores. Data moves between devices by JAX's collectives and lax.ppermute only.
A program may use at most 128 MiB of HBM per device.

```python
import math
import jax
import jax.numpy as jnp
import numpy as np
from jax import lax

D = 2048
ATTEND_GROUPS = 32
ATTEND_SIZE = 64
FF = 1024
SFF = 512
TOP = 2
TOK_A = 512
TOK_B = 128
TOKENS_A = 16384
TOKENS_B = 16384
EXPERTS = 32
CAP = 12
N_TP = 4


def slow_heads(key):
    chance = 0.5
    return jax.random.uniform(jax.random.fold_in(key, 101), (ATTEND_GROUPS,), jnp.float32) < chance


def draw_feature_forget_baseline(key, part):
    slow_mask = slow_heads(key)
    spread = jax.random.uniform(jax.random.fold_in(key, 202), (ATTEND_GROUPS, ATTEND_SIZE), jnp.float32)
    slow_log = jnp.log(0.05 / TOKENS_A) + spread * jnp.log(8.0)
    fast_log = jnp.log(0.01) + spread * jnp.log(100.0 / 30.0)
    return jnp.where(slow_mask[:, None], slow_log, fast_log).reshape(ATTEND_GROUPS * ATTEND_SIZE).astype(jnp.float32)


def draw_amend_speed_baseline(key, part):
    slow_mask = slow_heads(key)
    noise = jnp.clip(jax.random.normal(jax.random.fold_in(key, 303), (ATTEND_GROUPS, ATTEND_SIZE), jnp.float32), -3.0, 3.0)
    return jnp.where(slow_mask[:, None], -7.0 + 0.5 * noise, noise).reshape(ATTEND_GROUPS * ATTEND_SIZE).astype(jnp.float32)


def draw_forget_speed_dependent(key, part):
    block_count = TOKENS_A // TOK_A
    offsets = jax.random.uniform(jax.random.fold_in(key, 1), (block_count,), jnp.float32, -0.7, 0.7)
    noise = jnp.clip(0.6 * jax.random.normal(jax.random.fold_in(key, 2), (TOKENS_A, ATTEND_GROUPS * ATTEND_SIZE), jnp.float32), -2.0, 2.0)
    return (noise + jnp.repeat(offsets, TOK_A)[:, None]).astype(jnp.bfloat16)


def draw_sudden_forget_extra(key, part):
    where_at = jax.random.randint(jax.random.fold_in(key, 1), (2, 1, ATTEND_GROUPS), 0, TOKENS_A)
    losses = jax.random.uniform(jax.random.fold_in(key, 2), (2, 1, ATTEND_GROUPS), jnp.float32, jnp.log(0.6), jnp.log(0.8))
    row_ids = jnp.arange(TOKENS_A, dtype=jnp.int32)[None, :, None]
    return jnp.sum(jnp.where(row_ids == where_at, losses, 0.0), axis=0).astype(jnp.float32)


def block_levels(own_key, dims, pieces, low, high):
    level = 1.0
    for axis_at, parts in pieces:
        steps = jax.random.uniform(jax.random.fold_in(jax.random.fold_in(own_key, 6), axis_at), (parts,), jnp.float32, low / len(pieces), high / len(pieces))
        level = level * jnp.repeat(jnp.exp(steps), dims[axis_at] // parts).reshape((-1,) + (1,) * (len(dims) - 1 - axis_at))
    return level


def routed_block(rng, own, number, rows, count, top, reach, lean):
    ranking = jax.random.permutation(rng, count)
    heavy_load, common = load_shares(count, rows * top, reach, lean, True), load_shares(count, rows * top, reach, lean, False)
    places = jnp.arange(count)

    def named(sizes, offset_by):
        used = int((sizes > 0).sum())
        fixed = max(1, used // 4)
        shifted = fixed + (places - fixed + offset_by * (used - fixed)) % max(1, count - fixed)
        return jnp.zeros((count,), jnp.int32).at[ranking[jnp.where(places < fixed, places, shifted)]].set(jnp.asarray(sizes, jnp.int32))

    sizes = jnp.where(number % 4 == 0, named(heavy_load, number // 4), named(common, number - number // 4 - 1))
    mixed = jax.random.permutation(jax.random.fold_in(own, 3), count)
    source_of, receiver = mixed[0:count // 2 * 2:2], mixed[1:count // 2 * 2:2]
    room = jnp.minimum(sizes[source_of] - 1, reach - sizes[receiver]) // 2
    room = jnp.where((source_of == ranking[0]) | (receiver == ranking[0]) | (sizes[receiver] == 0), 0, jnp.maximum(room, 0))
    shifted = jax.random.randint(jax.random.fold_in(own, 4), (count // 2,), 0, 1 << 20) % (room + 1)
    sizes = sizes.at[source_of].add(-shifted).at[receiver].add(shifted)
    items = jnp.searchsorted(jnp.cumsum(sizes), jnp.arange(rows * top), side="right").astype(jnp.int32)
    table = items.reshape(top, rows).T
    table = table[jax.random.permutation(jax.random.fold_in(own, 1), rows)]
    offset_by = jax.random.randint(jax.random.fold_in(own, 2), (rows, 1), 0, top)
    return jnp.take_along_axis(table, (jnp.arange(top)[None, :] + offset_by) % top, axis=1)


def load_shares(number_of, total, bound, skew, full):
    loads = [(1 << 20) // math.isqrt(standing ** skew) + 1 for standing in range(1, number_of + 1)]
    largest = bound if full else min(bound, max(-(-total // number_of), total * loads[0] // sum(loads)))
    least = 1 if total - largest >= number_of - 1 else 0
    given, rest = [largest] + [least] * (number_of - 1), total - largest - least * (number_of - 1)
    while rest > 0:
        candidates = [i for i in range(1, number_of) if given[i] < largest] or [i for i in range(1, number_of) if given[i] < bound]
        mass, left = sum([loads[i] for i in candidates]), rest
        for i in candidates:
            extra = min(bound - given[i], max(1, left * loads[i] // mass), rest)
            given[i] = given[i] + extra
            rest = rest - extra
    return np.array(given)


def centred(rng, dims, width, reach, shards=(), kind=jnp.bfloat16):
    level = block_levels(rng, dims, shards, -0.22, 0.18) if shards else 1.0
    result = jax.random.normal(rng, dims, jnp.float32) * width * level
    return jnp.minimum(jnp.maximum(result, -reach), reach).astype(kind)


def setup_inputs(seed: int = 0, part: int = 0) -> dict:
    arg_keys = jax.random.split(jax.random.key(seed), 22)
    part_splits = jax.random.split(jax.random.fold_in(arg_keys[21], part), 22)
    query_vectors = centred(part_splits[0], (TOKENS_A, ATTEND_GROUPS * ATTEND_SIZE), 1.0, 6.0, ((0, 32), (1, 4)))
    attend_lookup_vectors = centred(part_splits[1], (TOKENS_A, ATTEND_GROUPS * ATTEND_SIZE), 1.0, 6.0, ((0, 32), (1, 4)))
    attend_content_vectors = centred(part_splits[2], (TOKENS_A, ATTEND_GROUPS * ATTEND_SIZE), 1.0, 6.0, ((0, 32), (1, 4)))
    forget_speed_dependent = draw_forget_speed_dependent(jax.random.fold_in(jax.random.fold_in(arg_keys[21], part), 71), part)
    amend_speed_dependent = centred(part_splits[4], (TOKENS_A, ATTEND_GROUPS * ATTEND_SIZE), 1.0, 6.0, ((0, 32), (1, 4)))
    result_switch_preactivation = centred(part_splits[5], (TOKENS_A, ATTEND_GROUPS * ATTEND_SIZE), 1.0, 6.0, ((0, 32), (1, 4)))
    feature_forget_baseline = draw_feature_forget_baseline(jax.random.fold_in(arg_keys[21], 71), part)
    amend_speed_baseline = draw_amend_speed_baseline(jax.random.fold_in(arg_keys[21], 71), part)
    sudden_forget_extra = draw_sudden_forget_extra(jax.random.fold_in(jax.random.fold_in(arg_keys[21], part), 71), part)
    group_scaling_factor = jnp.clip(1.0 + 0.18 * jax.random.normal(arg_keys[9], (ATTEND_GROUPS * ATTEND_SIZE,), jnp.float32), 0.1, 1.9)
    result_mapping_matrix = centred(arg_keys[10], (ATTEND_GROUPS * ATTEND_SIZE, D), (ATTEND_GROUPS * ATTEND_SIZE) ** -0.5, 0.125, ((0, 4),))
    specialist_tokens_activations = centred(part_splits[11], (TOKENS_B, D), 1.0, 6.0, ((0, 128),))
    specialist_scaling_factor = jnp.clip(1.0 + 0.18 * jax.random.normal(arg_keys[12], (D,), jnp.float32), 0.1, 1.9)
    selected_specialists_keys = jax.random.split(jax.random.fold_in(part_splits[13], 1), TOKENS_B // TOK_B)
    selected_specialists_turns = jax.random.permutation(jax.random.fold_in(part_splits[13], 3), TOKENS_B // TOK_B)
    selected_specialists = jax.vmap(lambda own, number: routed_block(jax.random.fold_in(part_splits[13], 2), own, number, TOK_B, EXPERTS, TOP, CAP, 2))(selected_specialists_keys, selected_specialists_turns).reshape((TOKENS_B, TOP))
    selection_mixing_factors = jnp.clip(jnp.exp(math.log(1.5) - 1.60943787 * jax.random.uniform(part_splits[14], (TOKENS_B, TOP), jnp.float32) ** block_levels(part_splits[14], (TOKENS_B, TOP), ((0, 128),), -0.2, 0.2)), 0.3, 1.5)
    dispatched_switch_matrix = centred(arg_keys[15], (EXPERTS, D, FF), D ** -0.5, 0.125, ((0, 32), (2, 4)))
    dispatched_raising_matrix = centred(arg_keys[16], (EXPERTS, D, FF), D ** -0.5, 0.125, ((0, 32), (2, 4)))
    dispatched_lowering_matrix = centred(arg_keys[17], (EXPERTS, FF, D), FF ** -0.5, 0.1875, ((0, 32), (1, 4)))
    common_switch_matrix = centred(arg_keys[18], (D, SFF), D ** -0.5, 0.125, ((1, 4),))
    common_raising_matrix = centred(arg_keys[19], (D, SFF), D ** -0.5, 0.125, ((1, 4),))
    common_lowering_matrix = centred(arg_keys[20], (SFF, D), SFF ** -0.5, 0.25, ((0, 4),))
    return dict(query_vectors=query_vectors, attend_lookup_vectors=attend_lookup_vectors, attend_content_vectors=attend_content_vectors, forget_speed_dependent=forget_speed_dependent, amend_speed_dependent=amend_speed_dependent, result_switch_preactivation=result_switch_preactivation, feature_forget_baseline=feature_forget_baseline, amend_speed_baseline=amend_speed_baseline, sudden_forget_extra=sudden_forget_extra, group_scaling_factor=group_scaling_factor, result_mapping_matrix=result_mapping_matrix, specialist_tokens_activations=specialist_tokens_activations, specialist_scaling_factor=specialist_scaling_factor, selected_specialists=selected_specialists, selection_mixing_factors=selection_mixing_factors, dispatched_switch_matrix=dispatched_switch_matrix, dispatched_raising_matrix=dispatched_raising_matrix, dispatched_lowering_matrix=dispatched_lowering_matrix, common_switch_matrix=common_switch_matrix, common_raising_matrix=common_raising_matrix, common_lowering_matrix=common_lowering_matrix)


highest = lax.Precision.HIGHEST

def split_sum(hidden, weight, blocks):
    width_dev = hidden.shape[1] // blocks
    summed = jnp.zeros((hidden.shape[0], weight.shape[1]), jnp.float32)
    for block_id in range(blocks):
        lower = block_id * width_dev
        partial_value = jnp.dot(hidden[:, lower:lower + width_dev], weight[lower:lower + width_dev], preferred_element_type=jnp.float32)
        summed = summed + lax.optimization_barrier(partial_value.astype(jnp.bfloat16)).astype(jnp.float32)
    return summed

def swiglu_rows(rows, gate_w, up_w):
    gate_vals = jnp.dot(rows, gate_w, preferred_element_type=jnp.float32)
    up_vals = jnp.dot(rows, up_w, preferred_element_type=jnp.float32)
    return (jax.nn.silu(gate_vals) * up_vals).astype(jnp.bfloat16)

def simple_attend_verify(query_vectors, attend_lookup_vectors, attend_content_vectors, forget_speed_dependent, amend_speed_dependent, result_switch_preactivation, feature_forget_baseline, amend_speed_baseline, sudden_forget_extra, group_scaling_factor, result_mapping_matrix):
    tokens = query_vectors.shape[0]

    def split_among_groups(array_in):
        return array_in.astype(jnp.float32).reshape(tokens, ATTEND_GROUPS, ATTEND_SIZE)
    forget_exponent_log = -jnp.exp(feature_forget_baseline.reshape(ATTEND_GROUPS, ATTEND_SIZE) + split_among_groups(forget_speed_dependent)) + sudden_forget_extra[:, :, None]
    learn_rate = jax.nn.sigmoid(amend_speed_baseline.reshape(ATTEND_GROUPS, ATTEND_SIZE) + split_among_groups(amend_speed_dependent))
    key_heads = split_among_groups(attend_lookup_vectors)
    unit_key = key_heads * lax.rsqrt(lax.optimization_barrier(jnp.sum(key_heads * key_heads, -1, keepdims=True)) + 1e-06)

    def advance(memory, inputs):
        recept_now, decay_now, write_now, value_now, unit_now, erase_now = inputs
        removed = jnp.einsum('hvk,hk->hv', memory, -unit_now, precision=highest)
        memory = memory * decay_now[:, None, :] + removed[:, :, None] * erase_now[:, None, :] + value_now[:, :, None] * write_now[:, None, :]
        return (memory, jnp.einsum('hvk,hk->hv', memory, recept_now, precision=highest))
    memory_zero = jnp.zeros((ATTEND_GROUPS, ATTEND_SIZE, ATTEND_SIZE), jnp.float32)
    memory_end, recur = lax.scan(advance, memory_zero, (split_among_groups(query_vectors), jnp.exp(forget_exponent_log), key_heads * learn_rate, split_among_groups(attend_content_vectors), unit_key, unit_key * learn_rate))
    head_mean = lax.optimization_barrier(jnp.mean(recur, -1, keepdims=True))
    centered = recur - head_mean
    head_var = lax.optimization_barrier(jnp.mean(centered * centered, -1, keepdims=True))
    normed = centered * lax.rsqrt(head_var + 0.00064) * group_scaling_factor.reshape(ATTEND_GROUPS, ATTEND_SIZE)
    mixed_rows = (normed * jax.nn.sigmoid(split_among_groups(result_switch_preactivation))).reshape(tokens, ATTEND_GROUPS * ATTEND_SIZE)
    mixed_rows = mixed_rows.astype(jnp.bfloat16)
    return split_sum(mixed_rows, result_mapping_matrix, N_TP).astype(jnp.bfloat16)

def moe_reference(specialist_tokens_activations, specialist_scaling_factor, selected_specialists, selection_mixing_factors, dispatched_switch_matrix, dispatched_raising_matrix, dispatched_lowering_matrix, common_switch_matrix, common_raising_matrix, common_lowering_matrix):
    floats = specialist_tokens_activations.astype(jnp.float32)
    normed = floats * lax.rsqrt(lax.optimization_barrier(jnp.mean(floats * floats, -1, keepdims=True)) + 1e-06) * specialist_scaling_factor
    normed = normed.astype(jnp.bfloat16)
    top_count = selected_specialists.shape[1]
    block_count = TOKENS_B // TOK_B
    flat_block = selected_specialists.reshape(block_count, TOK_B * top_count)
    one_hot = (flat_block[:, :, None] == jnp.arange(EXPERTS, dtype=jnp.int32)[None, None, :]).astype(jnp.int32)
    slot_rank = lax.optimization_barrier(jnp.sum((jnp.cumsum(one_hot, axis=1) - 1) * one_hot, axis=-1))
    position = (jnp.arange(block_count, dtype=jnp.int32)[:, None] * CAP + slot_rank).reshape(-1)
    flat_ids = flat_block.reshape(-1)
    weights_flat = selection_mixing_factors.reshape(-1)
    repeated = jnp.repeat(normed, top_count, axis=0)
    buffer_rows = block_count * CAP

    def per_expert(summed, operands):
        gate_w, up_w, down_w, expert_id = operands
        chosen = flat_ids == expert_id
        target = jnp.where(chosen, position, buffer_rows)
        buffer = jnp.zeros((buffer_rows, D), jnp.bfloat16).at[target].set(repeated, mode='drop')
        hidden = swiglu_rows(buffer, gate_w, up_w)
        expert_out = split_sum(hidden, down_w, N_TP).astype(jnp.bfloat16)
        picked = jnp.take(expert_out, jnp.minimum(position, buffer_rows - 1), axis=0).astype(jnp.float32)
        contrib = jnp.where(chosen[:, None], picked * weights_flat[:, None], 0.0)
        return (summed + lax.optimization_barrier(jnp.sum(contrib.reshape(TOKENS_B, top_count, D), axis=1)), None)
    routed, _ = lax.scan(per_expert, jnp.zeros((TOKENS_B, D), jnp.float32), (dispatched_switch_matrix, dispatched_raising_matrix, dispatched_lowering_matrix, jnp.arange(EXPERTS, dtype=jnp.int32)))
    shared_hidden = swiglu_rows(normed, common_switch_matrix, common_raising_matrix)
    shared_sum = split_sum(shared_hidden, common_lowering_matrix, N_TP)
    return (routed + shared_sum).astype(jnp.bfloat16)

def reference(query_vectors, attend_lookup_vectors, attend_content_vectors, forget_speed_dependent, amend_speed_dependent, result_switch_preactivation, feature_forget_baseline, amend_speed_baseline, sudden_forget_extra, group_scaling_factor, result_mapping_matrix, specialist_tokens_activations, specialist_scaling_factor, selected_specialists, selection_mixing_factors, dispatched_switch_matrix, dispatched_raising_matrix, dispatched_lowering_matrix, common_switch_matrix, common_raising_matrix, common_lowering_matrix):
    attend_result_matrix = simple_attend_verify(query_vectors, attend_lookup_vectors, attend_content_vectors, forget_speed_dependent, amend_speed_dependent, result_switch_preactivation, feature_forget_baseline, amend_speed_baseline, sudden_forget_extra, group_scaling_factor, result_mapping_matrix)
    moe_out = moe_reference(specialist_tokens_activations, specialist_scaling_factor, selected_specialists, selection_mixing_factors, dispatched_switch_matrix, dispatched_raising_matrix, dispatched_lowering_matrix, common_switch_matrix, common_raising_matrix, common_lowering_matrix)
    return (attend_result_matrix, moe_out)
```

```python
import jax
import jax.numpy as jnp
from jax import lax
from jax.experimental import pallas as pl
from jax.experimental.pallas import tpu as pltpu
from jax.sharding import PartitionSpec as P


F32 = jnp.float32
BF16 = jnp.bfloat16
SPAN = 64
VMEM_LIMIT = 56 * 1024 * 1024


def mm(a, b):
    return lax.dot_general(a, b, (((1,), (0,)), ((), ())), preferred_element_type=F32)


def mm_nt(a, b):
    return lax.dot_general(a, b, (((1,), (1,)), ((), ())), preferred_element_type=F32)


def mm_tn(a, b):
    return lax.dot_general(a, b, (((0,), (0,)), ((), ())), preferred_element_type=F32)


def iota(shape, dim):
    return lax.broadcasted_iota(jnp.int32, shape, dim)


def split_two(x):
    hi = x.astype(BF16)
    lo = (x - hi.astype(F32)).astype(BF16)
    return hi, lo


def sigmoid(x):
    return 1.0 / (1.0 + jnp.exp(-x))


def mixer_local(q_ref, k_ref, v_ref, f_ref, a_ref, x_ref, fb_ref, ab_ref, out_ref, q2_ref, ex_ref):
    tokens, width = q_ref.shape
    half = width // 2
    spans = tokens // SPAN
    parts = ex_ref.shape[0] // 2
    rows_per = half // parts
    pair = pl.program_id(0)
    lane = iota((SPAN, width), 1)
    row = iota((SPAN, width), 0)
    first = lane < half
    col = lane % half
    strict = row > col
    inclusive = row >= col
    eye = (row == col).astype(F32)
    tril = (iota((SPAN, SPAN), 0) >= iota((SPAN, SPAN), 1)).astype(BF16)
    ones_bd = ((iota((2 * width, width), 0) % width) // half == iota((2 * width, width), 1) // half).astype(BF16)
    levels = []
    size = 1
    while size < SPAN:
        levels.append(
            (row // (2 * size) == col // (2 * size)) & (row % (2 * size) >= size) & (col % (2 * size) < size)
        )
        size *= 2

    def bd(x):
        zero = jnp.zeros_like(x)
        return jnp.concatenate([jnp.where(first, x, zero), jnp.where(first, zero, x)], axis=0)

    heads = x_ref.shape[1]
    head_lane = iota((SPAN, heads), 1)
    fb = fb_ref[...]
    ab = ab_ref[...]

    def prepare(c):
        rows = pl.ds(c * SPAN, SPAN)
        extra = x_ref[rows, :]
        extra_a = jnp.sum(jnp.where(head_lane == 2 * pair, extra, 0.0), axis=1, keepdims=True)
        extra_b = jnp.sum(jnp.where(head_lane == 2 * pair + 1, extra, 0.0), axis=1, keepdims=True)
        decay = jnp.where(first, extra_a, extra_b) - jnp.exp(fb + f_ref[rows, :].astype(F32))
        hi = decay.astype(BF16)
        rest = decay - hi.astype(F32)
        mid = rest.astype(BF16)
        low = (rest - mid.astype(F32)).astype(BF16)
        sums = mm(tril, jnp.concatenate([hi, mid, low], axis=1))
        cum = sums[:, :width] + sums[:, width : 2 * width] + sums[:, 2 * width :]
        key = k_ref[rows, :].astype(F32)
        sq_hi, sq_lo = split_two(key * key)
        total = mm(jnp.concatenate([sq_hi, sq_lo], axis=1), ones_bd) + 1e-06
        inv = lax.rsqrt(total)
        unit = key * inv
        erase = unit * sigmoid(ab + a_ref[rows, :].astype(F32))
        scaled_value = v_ref[rows, :].astype(F32) * (total * inv)
        center = cum[SPAN // 2 : SPAN // 2 + 1, :]
        last = cum[SPAN - 1 : SPAN, :]
        left_erase = -unit * jnp.exp(cum - decay - center)
        left_read = q_ref[rows, :].astype(F32) * jnp.exp(cum - center)
        right = erase * jnp.exp(center - cum)
        pairs = mm_nt(jnp.concatenate([left_erase, left_read], axis=0).astype(BF16), bd(right.astype(BF16)))
        lower = jnp.where(strict, pairs[:SPAN], 0.0)
        read = jnp.where(inclusive, pairs[SPAN:], 0.0).astype(BF16)
        to_start = jnp.exp(center)
        rhs = jnp.concatenate(
            [bd(scaled_value.astype(BF16)), bd((left_erase * to_start).astype(BF16))], axis=1
        )
        read_start = left_read * to_start
        tail = (right * jnp.exp(last - center)).astype(BF16)
        return lower, read, rhs, read_start, tail, jnp.exp(last)

    state = jnp.concatenate([jnp.zeros((SPAN, width), F32), eye], axis=0)
    group = min(4, spans)
    for start in range(0, spans, group):
        prepared = [prepare(c) for c in range(start, start + group)]
        inverse = [eye + jnp.where(levels[0], p[0], 0.0) for p in prepared]
        for level in levels[1:]:
            packed = [x.astype(BF16) for x in inverse]
            step = [
                mm(x, bd(jnp.where(level, p[0], 0.0).astype(BF16))).astype(BF16)
                for x, p in zip(packed, prepared)
            ]
            inverse = [x + mm(y, bd(xb)) for x, y, xb in zip(inverse, step, packed)]
        solved = [mm(x.astype(BF16), p[2]).astype(BF16) for x, p in zip(inverse, prepared)]
        outs = [
            mm(p[1], jnp.concatenate([bd(u[:, :width]), bd(u[:, width:])], axis=1))
            for u, p in zip(solved, prepared)
        ]
        grams = [mm_tn(u, p[4]) for u, p in zip(solved, prepared)]
        for j in range(group):
            rows = pl.ds((start + j) * SPAN, SPAN)
            out, gram, prep = outs[j], grams[j], prepared[j]
            reads = (out[:, width:] + prep[3]).astype(BF16)
            state_b = state.astype(BF16)
            both = mm_nt(reads, jnp.concatenate([bd(state_b[:SPAN]), bd(state_b[SPAN:])], axis=0))
            out_ref[rows, :] = out[:, :width] + both[:, :width]
            q2_ref[rows, :] = both[:, width:].astype(BF16)
            add = jnp.where(first, gram[:SPAN], gram[SPAN : 2 * SPAN])
            trans = jnp.concatenate(
                [
                    jnp.where(first, gram[2 * SPAN : 3 * SPAN], 0.0),
                    jnp.where(first, 0.0, gram[3 * SPAN :]),
                ],
                axis=0,
            ).astype(BF16)
            state = state * prep[5] + mm(state_b, trans)
            state = jnp.concatenate([state[:SPAN] + add, state[SPAN:]], axis=0)
    offset = state[:SPAN]
    carry = state[SPAN:]
    offset_r = pltpu.roll(offset, half, 1)
    carry_r = pltpu.roll(carry, half, 1)
    h2 = SPAN // 2
    first_h = first[:h2]
    carry_a = jnp.where(first_h, carry[:h2], carry_r[h2:]).astype(BF16)
    carry_b = jnp.where(first_h, carry_r[:h2], carry[h2:]).astype(BF16)
    for head, (carried, added) in enumerate(((carry_a, offset), (carry_b, offset_r))):
        for part in range(parts):
            ex_ref[head * parts + part, 0:h2, :] = carried
            ex_ref[head * parts + part, h2 : h2 + rows_per, :] = added[
                part * rows_per : (part + 1) * rows_per
            ].astype(BF16)


def run_mixer_local(q, k, v, f, a, extra, fb, ab, holders):
    tokens, width = q.shape
    heads = extra.shape[1]
    head_size = width // heads
    pairs = heads // 2
    parts = holders // heads
    wide = 2 * head_size
    rows_per = head_size // parts
    ex_rows = head_size // 2 + rows_per
    spec = pl.BlockSpec((tokens, wide), lambda i: (0, i))
    vec = pl.BlockSpec((1, wide), lambda i: (0, i))
    return pl.pallas_call(
        mixer_local,
        grid=(pairs,),
        in_specs=[spec] * 5 + [pl.BlockSpec((tokens, heads), lambda i: (0, 0)), vec, vec],
        out_specs=[spec, spec, pl.BlockSpec((2 * parts, ex_rows, wide), lambda i: (i, 0, 0))],
        out_shape=[
            jax.ShapeDtypeStruct((tokens, width), F32),
            jax.ShapeDtypeStruct((tokens, width), BF16),
            jax.ShapeDtypeStruct((holders, ex_rows, wide), BF16),
        ],
        compiler_params=pltpu.CompilerParams(
            dimension_semantics=("arbitrary",), vmem_limit_bytes=VMEM_LIMIT
        ),
        cost_estimate=pl.CostEstimate(
            flops=40_000_000_000, transcendentals=2_000_000, bytes_accessed=5_000_000
        ),
        name="mixer_local",
    )(q, k, v, f, a, extra, fb.reshape(1, -1), ab.reshape(1, -1))


def chain_kernel(r_ref, o_ref):
    count, ex_rows, wide = r_ref.shape
    half = wide // 2
    h2 = half // 2
    rows_per = ex_rows - h2
    state = jnp.zeros((rows_per, half), F32)
    for d in range(count):
        block = r_ref[d]
        carried = jnp.concatenate([block[:h2, :half], block[:h2, half:]], axis=0)
        added = block[h2:, :half].astype(F32)
        state_b = state.astype(BF16)
        o_ref[d] = jnp.concatenate([state_b, state_b], axis=1)
        state = mm(state_b, carried) + added


def run_chain(received):
    count, ex_rows, wide = received.shape
    rows_per = ex_rows - wide // 4
    return pl.pallas_call(
        chain_kernel,
        out_shape=jax.ShapeDtypeStruct((count, rows_per, wide), BF16),
        cost_estimate=pl.CostEstimate(
            flops=3_000_000_000, transcendentals=0, bytes_accessed=600_000
        ),
        name="chain",
    )(received)


def mixer_final(me_ref, o_ref, q2_ref, s_ref, g_ref, gain_ref, w_ref, out_ref):
    width = o_ref.shape[1]
    wide = s_ref.shape[1]
    half = wide // 2
    pairs = width // wide
    first = iota((half, wide), 1) < half
    ones_bd = ((iota((2 * wide, wide), 0) % wide) // half == iota((2 * wide, wide), 1) // half).astype(BF16)

    def head_mean(x):
        hi, lo = split_two(x)
        return mm(jnp.concatenate([hi, lo], axis=1), ones_bd) * (1.0 / half)

    pieces = []
    for p in range(pairs):
        cols = slice(p * wide, (p + 1) * wide)
        state_a = s_ref[2 * p * half : (2 * p + 1) * half, :]
        state_b = s_ref[(2 * p + 1) * half : (2 * p + 2) * half, :]
        zero = jnp.zeros_like(state_a)
        both = jnp.concatenate([jnp.where(first, state_a, zero), jnp.where(first, zero, state_b)], axis=0)
        head_out = o_ref[:, cols] + mm_nt(q2_ref[:, cols], both)
        centered = head_out - head_mean(head_out)
        var = head_mean(centered * centered)
        gate = sigmoid(g_ref[:, cols].astype(F32))
        pieces.append((centered * lax.rsqrt(var + 0.00064) * gain_ref[:, cols] * gate).astype(BF16))
    mixed = jnp.concatenate(pieces, axis=1)
    out_ref[0] = mm(mixed, w_ref[...]).astype(BF16)


def run_mixer_final(me, out_local, q2, starts, at, wide, gate, gain, mapping, blocks):
    tokens, width = out_local.shape
    model = mapping.shape[1]
    rows = tokens // blocks

    def turned(i, me_ref):
        return ((me_ref[0] + i) % blocks, 0)

    spec = pl.BlockSpec((rows, width), turned)
    return pl.pallas_call(
        mixer_final,
        grid_spec=pltpu.PrefetchScalarGridSpec(
            num_scalar_prefetch=1,
            grid=(blocks,),
            in_specs=[
                spec,
                spec,
                pl.BlockSpec((starts.shape[0], wide), lambda i, me_ref: (0, at)),
                spec,
                pl.BlockSpec((1, width), lambda i, me_ref: (0, 0)),
                pl.BlockSpec((width, model), lambda i, me_ref: (0, 0)),
            ],
            out_specs=pl.BlockSpec((1, rows, model), lambda i, me_ref: (i, 0, 0)),
        ),
        out_shape=jax.ShapeDtypeStruct((blocks, rows, model), BF16),
        compiler_params=grid_params(),
        cost_estimate=pl.CostEstimate(
            flops=6_000_000_000, transcendentals=1_000_000, bytes_accessed=8_000_000
        ),
        name="mixer_final",
    )(me, out_local, q2, starts, gate, gain.reshape(1, -1), mapping)


def tail_pick(size, slot_rows, cap, third):
    r = iota((size, size), 0)
    c = iota((size, size), 1)
    s = r % slot_rows
    return (
        (r // slot_rows == c // slot_rows) & (s < cap) & (c % slot_rows == cap + s // 3) & (s % 3 == third)
    ).astype(BF16)


def dispatch_kernel(slot_rows, cap, t_ref, scale_ref, sel_ref, normed_ref, out_ref, pos_ref):
    rows, model = t_ref.shape
    total = out_ref.shape[0]
    main = out_ref.shape[1]
    third = main // 3
    experts = total // slot_rows
    floats = t_ref[...].astype(F32)
    mean = jnp.mean(floats * floats, axis=1, keepdims=True)
    normed = (floats * lax.rsqrt(mean + 1e-06) * scale_ref[...]).astype(BF16)
    wide = normed_ref.shape[1]
    for c in range(model // wide):
        normed_ref[c * rows : (c + 1) * rows, :] = normed[:, c * wide : (c + 1) * wide]
    ids = [sel_ref[:, 0:1], sel_ref[:, 1:2]]
    expert = iota((rows, experts), 1)
    hot = [(i == expert).astype(F32) for i in ids]
    strict = (iota((rows, rows), 0) > iota((rows, rows), 1)).astype(BF16)
    before = mm(strict, (hot[0] + hot[1]).astype(BF16))
    slots = [jnp.sum(h * before, axis=1, keepdims=True).astype(jnp.int32) for h in hot]
    place = iota((rows, total), 1)
    pos = [i * slot_rows + s for i, s in zip(ids, slots)]
    tail = [i * slot_rows + cap + s // 3 for i, s in zip(ids, slots)]
    which = [s % 3 for s in slots]
    pos_ref[...] = jnp.concatenate(pos, axis=1)
    main_hot = ((place == pos[0]) | (place == pos[1])).astype(BF16)
    for b in range(3):
        tail_hot = (
            ((place == tail[0]) & (which[0] == b)) | ((place == tail[1]) & (which[1] == b))
        ).astype(BF16)
        hot2 = jnp.concatenate([main_hot, tail_hot], axis=0)
        data = jnp.concatenate([normed[:, b * third : (b + 1) * third], normed[:, main:]], axis=0)
        out_ref[:, b * third : (b + 1) * third] = mm_tn(hot2, data).astype(BF16)


def hidden_kernel(slot_rows, cap, r_ref, g_ref, u_ref, h_ref, tail_ref):
    total, main = r_ref.shape
    third = main // 3
    size = min(256, total)

    @pl.when(pl.program_id(0) == 0)
    def _():
        for start in range(0, total, size):
            acc = jnp.zeros((size, third), F32)
            for b in range(3):
                acc = acc + mm(
                    tail_pick(size, slot_rows, cap, b), r_ref[start : start + size, b * third : (b + 1) * third]
                )
            tail_ref[start : start + size, :] = acc.astype(BF16)

    x = r_ref[...]
    t = tail_ref[...]
    gate = mm(x, g_ref[0, :main, :]) + mm(t, g_ref[0, main:, :])
    up = mm(x, u_ref[0, :main, :]) + mm(t, u_ref[0, main:, :])
    h_ref[...] = (gate * sigmoid(gate) * up).astype(BF16)


def lower_kernel(slot_rows, cap, h_ref, d_ref, t_ref, *refs):
    *extra, o_ref, tail_ref = refs
    total = h_ref.shape[0]
    third = d_ref.shape[2]
    size = min(256, total)
    b = pl.program_id(0)

    @pl.when(b == 0)
    def _():
        tail_ref[...] = mm(h_ref[...], t_ref[...].reshape(-1, third)).astype(BF16)
        for e_ref in extra:
            o_ref[:, 3 * third :] = e_ref[...]

    y = mm(h_ref[...], d_ref[...].reshape(-1, third))
    for start in range(0, total, size):
        moved = mm_tn(tail_pick(size, slot_rows, cap, b), tail_ref[start : start + size, :])
        slot = iota((size, third), 0) % slot_rows
        o_ref[start : start + size, pl.ds(pl.multiple_of(b * third, 128), third)] = jnp.where(
            slot < cap, y[start : start + size], moved
        ).astype(BF16)


def shared_kernel(me_ref, x_ref, g_ref, u_ref, d_ref, o_ref):
    rows = o_ref.shape[1]
    wide = x_ref.shape[2]
    gate = jnp.zeros((rows, g_ref.shape[1]), F32)
    up = jnp.zeros((rows, g_ref.shape[1]), F32)
    for c in range(x_ref.shape[1] // rows):
        x = x_ref[0, c * rows : (c + 1) * rows, :]
        gate = gate + mm(x, g_ref[c * wide : (c + 1) * wide, :])
        up = up + mm(x, u_ref[c * wide : (c + 1) * wide, :])
    hidden = (gate * sigmoid(gate) * up).astype(BF16)
    o_ref[0] = mm(hidden, d_ref[...]).astype(BF16)


def combine_kernel(slot_rows, cap, za_ref, zb_ref, pos_ref, mix_ref, s0_ref, s1_ref, s2_ref, s3_ref, o_ref):
    total, main = zb_ref.shape
    rows = pos_ref.shape[0]
    third = main // 3
    place = iota((rows, total), 1)
    pos = [pos_ref[:, 0:1], pos_ref[:, 1:2]]
    mix = [mix_ref[:, 0:1], mix_ref[:, 1:2]]
    slots = [p % slot_rows for p in pos]
    tail = [p - s + cap + s // 3 for p, s in zip(pos, slots)]
    which = [s % 3 for s in slots]
    weights = jnp.where(place == pos[0], mix[0], 0.0) + jnp.where(place == pos[1], mix[1], 0.0)
    w_hi, w_lo = split_two(weights)
    tails = []
    for b in range(3):
        tails.append(
            split_two(
                jnp.where((place == tail[0]) & (which[0] == b), mix[0], 0.0)
                + jnp.where((place == tail[1]) & (which[1] == b), mix[1], 0.0)
            )
        )

    def shared(cols):
        acc = s0_ref[:, cols].astype(F32)
        for other in (s1_ref, s2_ref, s3_ref):
            acc = acc + other[:, cols].astype(F32)
        return acc

    for half, z_ref in enumerate((za_ref, zb_ref)):
        base = half * (main + third)
        tail_sum = jnp.zeros((rows, third), F32)
        for b in range(3):
            cols = slice(base + b * third, base + (b + 1) * third)
            z = z_ref[:, b * third : (b + 1) * third]
            o_ref[:, cols] = (mm(w_hi, z) + mm(w_lo, z) + shared(cols)).astype(BF16)
            tail_sum = tail_sum + mm(tails[b][0], z) + mm(tails[b][1], z)
        cols = slice(base + main, base + main + third)
        o_ref[:, cols] = (tail_sum + shared(cols)).astype(BF16)


def bind(kernel, *static):
    def body(*refs):
        kernel(*static, *refs)

    body.__name__ = kernel.__name__
    return body


def params():
    return pltpu.CompilerParams(vmem_limit_bytes=VMEM_LIMIT)


def grid_params():
    return pltpu.CompilerParams(dimension_semantics=("arbitrary",), vmem_limit_bytes=VMEM_LIMIT)


def turn_exchange(x, axis):
    count = x.shape[0]
    out = [x[0]]
    for d in range(1, count):
        out.append(lax.ppermute(x[d], axis, [(i, (i + d) % count) for i in range(count)]))
    return out


def exchange(x, axis):
    return lax.all_to_all(x, axis, split_axis=0, concat_axis=0, tiled=True)


def on_device(
    query_vectors,
    attend_lookup_vectors,
    attend_content_vectors,
    forget_speed_dependent,
    amend_speed_dependent,
    result_switch_preactivation,
    feature_forget_baseline,
    amend_speed_baseline,
    sudden_forget_extra,
    group_scaling_factor,
    result_mapping_matrix,
    specialist_tokens_activations,
    specialist_scaling_factor,
    selected_specialists,
    selection_mixing_factors,
    dispatched_switch_matrix,
    dispatched_raising_matrix,
    dispatched_lowering_matrix,
    common_switch_matrix,
    common_raising_matrix,
    common_lowering_matrix,
):
    tok_rows, top_count = selected_specialists.shape
    model = specialist_tokens_activations.shape[1]
    experts = lax.axis_size("ep")
    tp_size = lax.axis_size("tp")
    cap = 3 * tok_rows * top_count // (2 * experts)
    slot_rows = cap * 4 // 3
    main = model * 3 // 4
    third = model // 4
    total = experts * slot_rows

    ff = dispatched_switch_matrix.shape[2]
    half_model = model // 2
    half_main = main // 2
    half_third = third // 2
    low_blocks = half_model // ff

    def stacked(x):
        return x.reshape(ff, low_blocks, ff).transpose(1, 0, 2).reshape(low_blocks * ff, ff)

    lowering = dispatched_lowering_matrix[0]
    early = lax.all_gather(
        jnp.concatenate(
            [
                dispatched_switch_matrix[0],
                dispatched_raising_matrix[0],
                stacked(lowering[:, :half_model]),
            ],
            axis=0,
        ),
        "tp",
    )

    normed, outgoing, positions = pl.pallas_call(
        bind(dispatch_kernel, slot_rows, cap),
        out_shape=[
            jax.ShapeDtypeStruct((tok_rows * model // ff, ff), BF16),
            jax.ShapeDtypeStruct((total, main), BF16),
            jax.ShapeDtypeStruct((tok_rows, top_count), jnp.int32),
        ],
        compiler_params=params(),
        name="dispatch",
    )(specialist_tokens_activations, specialist_scaling_factor.reshape(1, -1), selected_specialists)

    late = lax.all_gather(
        jnp.concatenate([stacked(lowering[:, half_model:]), normed], axis=0), "tp"
    )

    received = exchange(outgoing.reshape(experts, slot_rows, main), "ep").reshape(total, main)

    out_local, q2, outgoing_state = run_mixer_local(
        query_vectors,
        attend_lookup_vectors,
        attend_content_vectors,
        forget_speed_dependent,
        amend_speed_dependent,
        sudden_forget_extra,
        feature_forget_baseline,
        amend_speed_baseline,
        experts,
    )
    states = exchange(outgoing_state, "ep")
    chained = run_chain(states)
    chained = chained.reshape(-1, chained.shape[2])
    wide = chained.shape[1]

    hidden = pl.pallas_call(
        bind(hidden_kernel, slot_rows, cap),
        grid=(tp_size,),
        in_specs=[
            pl.BlockSpec((total, main), lambda i: (0, 0)),
            pl.BlockSpec((1, model, ff), lambda i: (i, 0, 0)),
            pl.BlockSpec((1, model, ff), lambda i: (i, 1, 0)),
        ],
        out_specs=pl.BlockSpec((total, ff), lambda i: (0, i)),
        out_shape=jax.ShapeDtypeStruct((total, ff * tp_size), BF16),
        scratch_shapes=[pltpu.VMEM((total, third), BF16)],
        compiler_params=grid_params(),
        name="hidden",
    )(received, early, early)

    def lower(weights, base, *extra):
        out_width = half_main + sum(e.shape[1] for e in extra)
        return pl.pallas_call(
            bind(lower_kernel, slot_rows, cap),
            grid=(3,),
            in_specs=[
                pl.BlockSpec((total, ff * tp_size), lambda i: (0, 0)),
                pl.BlockSpec((tp_size, ff, half_third), lambda i: (0, base + i, 0)),
                pl.BlockSpec((tp_size, ff, half_third), lambda i: (0, base + 3, 0)),
            ]
            + [pl.BlockSpec(e.shape, lambda i: (0, 0)) for e in extra],
            out_specs=pl.BlockSpec((total, out_width), lambda i: (0, 0)),
            out_shape=jax.ShapeDtypeStruct((total, out_width), BF16),
            scratch_shapes=[pltpu.VMEM((total, half_third), BF16)],
            compiler_params=grid_params(),
            name="lower",
        )(hidden, weights, weights, *extra)

    def send_back(x):
        return exchange(x.reshape(experts, slot_rows, x.shape[1]), "ep").reshape(x.shape)

    first_half = lower(early, 2 * model // ff, chained)
    first_back = send_back(first_half)
    second_half = lower(late, 0)
    second_back = send_back(second_half)

    me = lax.axis_index("tp").astype(jnp.int32).reshape(1)
    sff = common_switch_matrix.shape[1]
    shared_part = pl.pallas_call(
        shared_kernel,
        grid_spec=pltpu.PrefetchScalarGridSpec(
            num_scalar_prefetch=1,
            grid=(tp_size,),
            in_specs=[
                pl.BlockSpec(
                    (1, tok_rows * model // ff, ff), lambda i, me_ref: ((me_ref[0] + i) % tp_size, 1, 0)
                ),
                pl.BlockSpec((model, sff), lambda i, me_ref: (0, 0)),
                pl.BlockSpec((model, sff), lambda i, me_ref: (0, 0)),
                pl.BlockSpec((sff, model), lambda i, me_ref: (0, 0)),
            ],
            out_specs=pl.BlockSpec((1, tok_rows, model), lambda i, me_ref: (i, 0, 0)),
        ),
        out_shape=jax.ShapeDtypeStruct((tp_size, tok_rows, model), BF16),
        compiler_params=grid_params(),
        name="shared",
    )(me, late, common_switch_matrix, common_raising_matrix, common_lowering_matrix)
    shared_blocks = turn_exchange(shared_part, "tp")

    mixed_part = run_mixer_final(
        me,
        out_local,
        q2,
        first_back,
        half_main // wide,
        wide,
        result_switch_preactivation,
        group_scaling_factor,
        result_mapping_matrix,
        tp_size,
    )
    mixed_blocks = turn_exchange(mixed_part, "tp")
    mixed_sum = mixed_blocks[0].astype(F32)
    for block in mixed_blocks[1:]:
        mixed_sum = mixed_sum + block.astype(F32)
    attend_result_matrix = mixed_sum.astype(BF16)
    moe_out = pl.pallas_call(
        bind(combine_kernel, slot_rows, cap),
        out_shape=jax.ShapeDtypeStruct((tok_rows, model), BF16),
        compiler_params=params(),
        name="combine",
    )(first_back, second_back, positions, selection_mixing_factors, *shared_blocks)
    return (attend_result_matrix, moe_out)


def solution(mesh):
    by_rows = P(("grp", "ep"), "tp")
    by_device = P(("grp", "ep", "tp"), None)
    placed = (
        by_rows,
        by_rows,
        by_rows,
        by_rows,
        by_rows,
        by_rows,
        P("tp"),
        P("tp"),
        by_rows,
        P("tp"),
        P("tp", None),
        by_device,
        P(),
        by_device,
        by_device,
        P("ep", None, "tp"),
        P("ep", None, "tp"),
        P("ep", "tp", None),
        P(None, "tp"),
        P(None, "tp"),
        P("tp", None),
    )
    return jax.shard_map(
        on_device, mesh=mesh, in_specs=placed, out_specs=(by_device, by_device), check_vma=False
    )
```

```python
import jax
import jax.numpy as jnp
from jax import lax
from jax.experimental import pallas as pl
from jax.experimental.pallas import tpu as pltpu
from jax.sharding import PartitionSpec as P


F32 = jnp.float32
BF16 = jnp.bfloat16
SPAN = 64
VMEM_LIMIT = 56 * 1024 * 1024


def mm(a, b):
    return lax.dot_general(a, b, (((1,), (0,)), ((), ())), preferred_element_type=F32)


def mm_nt(a, b):
    return lax.dot_general(a, b, (((1,), (1,)), ((), ())), preferred_element_type=F32)


def mm_tn(a, b):
    return lax.dot_general(a, b, (((0,), (0,)), ((), ())), preferred_element_type=F32)


def iota(shape, dim):
    return lax.broadcasted_iota(jnp.int32, shape, dim)


def split_two(x):
    hi = x.astype(BF16)
    lo = (x - hi.astype(F32)).astype(BF16)
    return hi, lo


def sigmoid(x):
    return 1.0 / (1.0 + jnp.exp(-x))


def mixer_local(q_ref, k_ref, v_ref, f_ref, a_ref, x_ref, fb_ref, ab_ref, out_ref, q2_ref, ex_ref, state_ref):
    tokens, width = q_ref.shape
    half = width // 2
    spans = tokens // SPAN
    pair = pl.program_id(0)
    lane = iota((SPAN, width), 1)
    row = iota((SPAN, width), 0)
    first = lane < half
    col = lane % half
    strict = row > col
    inclusive = row >= col
    eye = (row == col).astype(F32)
    tril = (iota((SPAN, SPAN), 0) >= iota((SPAN, SPAN), 1)).astype(BF16)
    ones_bd = ((iota((2 * width, width), 0) % width) // half == iota((2 * width, width), 1) // half).astype(BF16)
    levels = []
    size = 1
    while size < SPAN:
        levels.append(
            (row // (2 * size) == col // (2 * size)) & (row % (2 * size) >= size) & (col % (2 * size) < size)
        )
        size *= 2

    def bd(x):
        zero = jnp.zeros_like(x)
        return jnp.concatenate([jnp.where(first, x, zero), jnp.where(first, zero, x)], axis=0)

    heads = x_ref.shape[1]
    head_lane = iota((SPAN, heads), 1)
    fb = fb_ref[...]
    ab = ab_ref[...]

    def prepare(c):
        rows = pl.ds(pl.multiple_of(c * SPAN, SPAN), SPAN)
        extra = x_ref[rows, :]
        extra_a = jnp.sum(jnp.where(head_lane == 2 * pair, extra, 0.0), axis=1, keepdims=True)
        extra_b = jnp.sum(jnp.where(head_lane == 2 * pair + 1, extra, 0.0), axis=1, keepdims=True)
        decay = jnp.where(first, extra_a, extra_b) - jnp.exp(fb + f_ref[rows, :].astype(F32))
        hi = decay.astype(BF16)
        rest = decay - hi.astype(F32)
        mid = rest.astype(BF16)
        low = (rest - mid.astype(F32)).astype(BF16)
        sums = mm(tril, jnp.concatenate([hi, mid, low], axis=1))
        cum = sums[:, :width] + sums[:, width : 2 * width] + sums[:, 2 * width :]
        key = k_ref[rows, :].astype(F32)
        sq_hi, sq_lo = split_two(key * key)
        total = mm(jnp.concatenate([sq_hi, sq_lo], axis=1), ones_bd) + 1e-06
        inv = lax.rsqrt(total)
        unit = key * inv
        erase = unit * sigmoid(ab + a_ref[rows, :].astype(F32))
        scaled_value = v_ref[rows, :].astype(F32) * (total * inv)
        center = cum[SPAN // 2 : SPAN // 2 + 1, :]
        last = cum[SPAN - 1 : SPAN, :]
        left_erase = -unit * jnp.exp(cum - decay - center)
        left_read = q_ref[rows, :].astype(F32) * jnp.exp(cum - center)
        right = erase * jnp.exp(center - cum)
        pairs = mm_nt(jnp.concatenate([left_erase, left_read], axis=0).astype(BF16), bd(right.astype(BF16)))
        lower = jnp.where(strict, pairs[:SPAN], 0.0)
        read = jnp.where(inclusive, pairs[SPAN:], 0.0).astype(BF16)
        to_start = jnp.exp(center)
        rhs = jnp.concatenate(
            [bd(scaled_value.astype(BF16)), bd((left_erase * to_start).astype(BF16))], axis=1
        )
        read_start = left_read * to_start
        tail = (right * jnp.exp(last - center)).astype(BF16)
        return lower, read, rhs, read_start, tail, jnp.exp(last)

    state_ref[...] = jnp.concatenate([jnp.zeros((SPAN, width), F32), eye], axis=0)
    group = min(4, spans)

    @pl.loop(0, spans // group)
    def _(turn):
        start = turn * group
        state = state_ref[...]
        prepared = [prepare(start + j) for j in range(group)]
        inverse = [eye + jnp.where(levels[0], p[0], 0.0) for p in prepared]
        for level in levels[1:]:
            packed = [x.astype(BF16) for x in inverse]
            step = [
                mm(x, bd(jnp.where(level, p[0], 0.0).astype(BF16))).astype(BF16)
                for x, p in zip(packed, prepared)
            ]
            inverse = [x + mm(y, bd(xb)) for x, y, xb in zip(inverse, step, packed)]
        solved = [mm(x.astype(BF16), p[2]).astype(BF16) for x, p in zip(inverse, prepared)]
        outs = [
            mm(p[1], jnp.concatenate([bd(u[:, :width]), bd(u[:, width:])], axis=1))
            for u, p in zip(solved, prepared)
        ]
        grams = [mm_tn(u, p[4]) for u, p in zip(solved, prepared)]
        for j in range(group):
            rows = pl.ds(pl.multiple_of((start + j) * SPAN, SPAN), SPAN)
            out, gram, prep = outs[j], grams[j], prepared[j]
            reads = (out[:, width:] + prep[3]).astype(BF16)
            state_b = state.astype(BF16)
            both = mm_nt(reads, jnp.concatenate([bd(state_b[:SPAN]), bd(state_b[SPAN:])], axis=0))
            out_ref[rows, :] = out[:, :width] + both[:, :width]
            q2_ref[rows, :] = both[:, width:].astype(BF16)
            add = jnp.where(first, gram[:SPAN], gram[SPAN : 2 * SPAN])
            trans = jnp.concatenate(
                [
                    jnp.where(first, gram[2 * SPAN : 3 * SPAN], 0.0),
                    jnp.where(first, 0.0, gram[3 * SPAN :]),
                ],
                axis=0,
            ).astype(BF16)
            state = state * prep[5] + mm(state_b, trans)
            state = jnp.concatenate([state[:SPAN] + add, state[SPAN:]], axis=0)
        state_ref[...] = state

    ex_ref[...] = state_ref[...].astype(BF16)


def run_mixer_local(q, k, v, f, a, extra, fb, ab):
    tokens, width = q.shape
    heads = extra.shape[1]
    head_size = width // heads
    pairs = heads // 2
    wide = 2 * head_size
    spec = pl.BlockSpec((tokens, wide), lambda i: (0, i))
    vec = pl.BlockSpec((1, wide), lambda i: (0, i))
    return pl.pallas_call(
        mixer_local,
        grid=(pairs,),
        in_specs=[spec] * 5 + [pl.BlockSpec((tokens, heads), lambda i: (0, 0)), vec, vec],
        out_specs=[spec, spec, pl.BlockSpec((wide, wide), lambda i: (i, 0))],
        out_shape=[
            jax.ShapeDtypeStruct((tokens, width), F32),
            jax.ShapeDtypeStruct((tokens, width), BF16),
            jax.ShapeDtypeStruct((pairs * wide, wide), BF16),
        ],
        scratch_shapes=[pltpu.VMEM((2 * SPAN, wide), F32)],
        compiler_params=pltpu.CompilerParams(
            dimension_semantics=("arbitrary",), vmem_limit_bytes=VMEM_LIMIT
        ),
        cost_estimate=pl.CostEstimate(
            flops=40_000_000_000, transcendentals=2_000_000, bytes_accessed=5_000_000
        ),
        name="mixer_local",
    )(q, k, v, f, a, extra, fb.reshape(1, -1), ab.reshape(1, -1))


def chain_kernel(me_ref, r_ref, o_ref, state_ref):
    rows, wide = r_ref.shape[1:]
    half = wide // 2
    pairs = rows // wide
    first = iota((half, wide), 1) < half
    state_ref[...] = jnp.zeros_like(state_ref)

    @pl.loop(0, r_ref.shape[0])
    def _(d):
        @pl.when(d < me_ref[0])
        def _():
            for p in range(pairs):
                own = slice(p * half, (p + 1) * half)
                added = r_ref[d, p * wide : p * wide + half, :].astype(F32)
                carried = r_ref[d, p * wide + half : (p + 1) * wide, :]
                zero = jnp.zeros_like(carried)
                carried = jnp.concatenate(
                    [jnp.where(first, carried, zero), jnp.where(first, zero, carried)], axis=0
                )
                state_ref[own, :] = mm(state_ref[own, :].astype(BF16), carried) + added

    o_ref[...] = state_ref[...].astype(BF16)


def run_chain(me, gathered):
    _, rows, wide = gathered.shape
    return pl.pallas_call(
        chain_kernel,
        grid_spec=pltpu.PrefetchScalarGridSpec(
            num_scalar_prefetch=1,
            grid=(1,),
            in_specs=[pl.BlockSpec(gathered.shape, lambda i, me_ref: (0, 0, 0))],
            out_specs=pl.BlockSpec((rows // 2, wide), lambda i, me_ref: (0, 0)),
            scratch_shapes=[pltpu.VMEM((rows // 2, wide), F32)],
        ),
        out_shape=jax.ShapeDtypeStruct((rows // 2, wide), BF16),
        compiler_params=grid_params(),
        cost_estimate=pl.CostEstimate(
            flops=3_000_000_000, transcendentals=0, bytes_accessed=4_000_000
        ),
        name="chain",
    )(me, gathered)


def mixer_final(me_ref, o_ref, q2_ref, s_ref, g_ref, gain_ref, w_ref, *outs):
    width = o_ref.shape[1]
    wide = s_ref.shape[1]
    half = wide // 2
    pairs = width // wide
    first = iota((half, wide), 1) < half
    ones_bd = ((iota((2 * wide, wide), 0) % wide) // half == iota((2 * wide, wide), 1) // half).astype(BF16)

    def head_mean(x):
        hi, lo = split_two(x)
        return mm(jnp.concatenate([hi, lo], axis=1), ones_bd) * (1.0 / half)

    pieces = []
    for p in range(pairs):
        cols = slice(p * wide, (p + 1) * wide)
        state = s_ref[p * half : (p + 1) * half, :]
        zero = jnp.zeros_like(state)
        both = jnp.concatenate([jnp.where(first, state, zero), jnp.where(first, zero, state)], axis=0)
        head_out = o_ref[:, cols] + mm_nt(q2_ref[:, cols], both)
        centered = head_out - head_mean(head_out)
        var = head_mean(centered * centered)
        gate = sigmoid(g_ref[:, cols].astype(F32))
        pieces.append((centered * lax.rsqrt(var + 0.00064) * gain_ref[:, cols] * gate).astype(BF16))
    mixed = jnp.concatenate(pieces, axis=1)
    result = mm(mixed, w_ref[...]).astype(BF16)
    for d, out_ref in enumerate(outs):

        @pl.when(pl.program_id(0) == d)
        def _(out_ref=out_ref):
            out_ref[...] = result


def run_mixer_final(me, out_local, q2, starts, gate, gain, mapping, blocks):
    tokens, width = out_local.shape
    model = mapping.shape[1]
    rows = tokens // blocks

    def turned(i, me_ref):
        return ((me_ref[0] + i) % blocks, 0)

    spec = pl.BlockSpec((rows, width), turned)
    return pl.pallas_call(
        mixer_final,
        grid_spec=pltpu.PrefetchScalarGridSpec(
            num_scalar_prefetch=1,
            grid=(blocks,),
            in_specs=[
                spec,
                spec,
                pl.BlockSpec(starts.shape, lambda i, me_ref: (0, 0)),
                spec,
                pl.BlockSpec((1, width), lambda i, me_ref: (0, 0)),
                pl.BlockSpec((width, model), lambda i, me_ref: (0, 0)),
            ],
            out_specs=[pl.BlockSpec((rows, model), lambda i, me_ref: (0, 0))] * blocks,
        ),
        out_shape=[jax.ShapeDtypeStruct((rows, model), BF16)] * blocks,
        compiler_params=grid_params(),
        cost_estimate=pl.CostEstimate(
            flops=6_000_000_000, transcendentals=1_000_000, bytes_accessed=8_000_000
        ),
        name="mixer_final",
    )(me, out_local, q2, starts, gate, gain.reshape(1, -1), mapping)


def picks(size, slot_rows, cap):
    kept = size // slot_rows * cap
    r = iota((kept, 1), 0)
    block = r // cap
    s = r - block * cap
    c = iota((kept, size), 1)
    at_tail = c == block * slot_rows + cap + s // 3
    return (c == block * slot_rows + s).astype(BF16), [
        (at_tail & (s % 3 == third)).astype(BF16) for third in range(3)
    ]


def dispatch_kernel(slot_rows, cap, t_ref, scale_ref, sel_ref, normed_ref, out_ref, pos_ref):
    rows, _ = t_ref.shape
    total = out_ref.shape[0]
    main = out_ref.shape[1]
    third = main // 3
    experts = total // slot_rows
    floats = t_ref[...].astype(F32)
    mean = jnp.mean(floats * floats, axis=1, keepdims=True)
    normed = (floats * lax.rsqrt(mean + 1e-06) * scale_ref[...]).astype(BF16)
    normed_ref[...] = normed
    named = sel_ref[...].astype(F32)
    named = jnp.concatenate([named] * (8 // named.shape[0]), axis=0).T.astype(jnp.int32)
    ids = [named[:, 0:1], named[:, 1:2]]
    expert = iota((rows, experts), 1)
    hot = [(i == expert).astype(F32) for i in ids]
    strict = (iota((rows, rows), 0) > iota((rows, rows), 1)).astype(BF16)
    before = mm(strict, (hot[0] + hot[1]).astype(BF16))
    slots = [jnp.sum(h * before, axis=1, keepdims=True).astype(jnp.int32) for h in hot]
    place = iota((rows, total), 1)
    pos = [i * slot_rows + s for i, s in zip(ids, slots)]
    tail = [i * slot_rows + cap + s // 3 for i, s in zip(ids, slots)]
    which = [s % 3 for s in slots]
    pos_ref[...] = jnp.concatenate(pos, axis=1)
    main_hot = ((place == pos[0]) | (place == pos[1])).astype(BF16)
    for b in range(3):
        tail_hot = (
            ((place == tail[0]) & (which[0] == b)) | ((place == tail[1]) & (which[1] == b))
        ).astype(BF16)
        hot2 = jnp.concatenate([main_hot, tail_hot], axis=0)
        data = jnp.concatenate([normed[:, b * third : (b + 1) * third], normed[:, main:]], axis=0)
        out_ref[:, b * third : (b + 1) * third] = mm_tn(hot2, data).astype(BF16)


class Copies:
    def __init__(self, sems):
        self.sems = sems
        self.made = []

    def start(self, src, dst, group):
        copy = pltpu.make_async_copy(src, dst, self.sems.at[len(self.made)])
        copy.start()
        self.made.append((group, copy))

    def wait(self, group):
        for at, copy in self.made:
            if at == group:
                copy.wait()


def near_kernel(slot_rows, cap, r_ref, *refs):
    blocks = (len(refs) - 5) // 2
    gates, ups = refs[:blocks], refs[blocks : 2 * blocks]
    h_ref, x_ref, g_ref, u_ref, sems = refs[2 * blocks :]
    total, main = r_ref.shape
    third = main // 3
    ff = g_ref.shape[2]
    size = min(256, total)
    kept = size // slot_rows * cap
    copies = Copies(sems)
    for k in range(blocks):
        copies.start(gates[k], g_ref.at[k], k)
        copies.start(ups[k], u_ref.at[k], k)
    whole, tails = picks(size, slot_rows, cap)
    for i in range(total // size):
        rows = slice(i * kept, (i + 1) * kept)
        block = r_ref[i * size : (i + 1) * size, :]
        x_ref[rows, :main] = mm(whole, block).astype(BF16)
        acc = jnp.zeros((kept, third), F32)
        for b in range(3):
            acc = acc + mm(tails[b], block[:, b * third : (b + 1) * third])
        x_ref[rows, main:] = acc.astype(BF16)
    for k in range(blocks):
        copies.wait(k)
        gate = mm(x_ref[...], g_ref[k])
        up = mm(x_ref[...], u_ref[k])
        h_ref[:, k * ff : (k + 1) * ff] = (gate * sigmoid(gate) * up).astype(BF16)


def far_kernel(slot_rows, cap, x_hbm, h_hbm, fa, fb, *refs):
    *downs, o_ref, x_ref, h_ref, g_ref, u_ref, d_ref, tail_ref, sems = refs
    total, main = o_ref.shape
    third = main // 3
    model, ff = g_ref.shape
    near = h_ref.shape[1] - ff
    half = model // 2
    size = min(256, total)
    kept = size // slot_rows * cap
    copies = Copies(sems)
    copies.start(x_hbm, x_ref, "x")
    for src, at in ((fa, 0), (fb, half)):
        copies.start(src.at[0:half, :], g_ref.at[at : at + half, :], "x")
        copies.start(src.at[half:model, :], u_ref.at[at : at + half, :], "x")
    copies.start(h_hbm, h_ref.at[:, 0:near], "d")
    base = 0
    for src in downs:
        rows = src.shape[0]
        copies.start(src, d_ref.at[base : base + rows, :], "d")
        base += rows
    whole, tails = picks(size, slot_rows, cap)
    copies.wait("x")
    gate = mm(x_ref[...], g_ref[...])
    up = mm(x_ref[...], u_ref[...])
    copies.wait("d")
    h_ref[:, near:] = (gate * sigmoid(gate) * up).astype(BF16)
    tail_ref[...] = mm(h_ref[...], d_ref[:, main:]).astype(BF16)
    for b in range(3):
        cols = slice(b * third, (b + 1) * third)
        y = mm(h_ref[...], d_ref[:, cols]).astype(BF16)
        spread = jnp.concatenate([whole, tails[b]], axis=0)
        for i in range(total // size):
            rows = slice(i * kept, (i + 1) * kept)
            both = jnp.concatenate([y[rows], tail_ref[rows, :]], axis=0)
            o_ref[i * size : (i + 1) * size, cols] = mm_tn(spread, both).astype(BF16)


def shared_kernel(*refs):
    count = (len(refs) - 3) // 2
    rows_in, outs = refs[:count], refs[count + 3 :]
    g_ref, u_ref, d_ref = refs[count : count + 3]
    x = jnp.concatenate([ref[...] for ref in rows_in], axis=0)
    gate = mm(x, g_ref[...])
    up = mm(x, u_ref[...])
    hidden = (gate * sigmoid(gate) * up).astype(BF16)
    for d, o_ref in enumerate(outs):
        rows = o_ref.shape[0]
        o_ref[...] = mm(hidden[d * rows : (d + 1) * rows], d_ref[...]).astype(BF16)


def prepare_kernel(slot_rows, cap, pos_ref, mix_ref, *refs):
    *blocks, w_ref, base_ref = refs
    rows = pos_ref.shape[0]
    place = iota((rows, w_ref.shape[1]), 1)
    pos = [pos_ref[:, 0:1], pos_ref[:, 1:2]]
    mix = [mix_ref[:, 0:1], mix_ref[:, 1:2]]
    slots = [p % slot_rows for p in pos]
    tail = [p - s + cap + s // 3 for p, s in zip(pos, slots)]
    which = [s % 3 for s in slots]
    main = jnp.where(place == pos[0], mix[0], 0.0) + jnp.where(place == pos[1], mix[1], 0.0)
    main = main.astype(BF16)
    for b in range(3):
        w_ref[2 * b * rows : (2 * b + 1) * rows, :] = main
        w_ref[(2 * b + 1) * rows : (2 * b + 2) * rows, :] = (
            jnp.where((place == tail[0]) & (which[0] == b), mix[0], 0.0)
            + jnp.where((place == tail[1]) & (which[1] == b), mix[1], 0.0)
        ).astype(BF16)
    base = blocks[0][...].astype(F32)
    for block in blocks[1:]:
        base = base + block[...].astype(F32)
    base_ref[...] = base


def combine_kernel(z_ref, w_ref, base_ref, o_ref):
    main = z_ref.shape[1]
    rows = o_ref.shape[0]
    third = main // 3
    tail_sum = base_ref[:, main:]
    for b in range(3):
        cols = slice(b * third, (b + 1) * third)
        both = mm(w_ref[2 * b * rows : 2 * (b + 1) * rows, :], z_ref[:, cols])
        o_ref[:, cols] = (base_ref[:, cols] + both[:rows]).astype(BF16)
        tail_sum = tail_sum + both[rows:]
    o_ref[:, main:] = tail_sum.astype(BF16)


def bind(kernel, *static):
    def body(*refs):
        kernel(*static, *refs)

    body.__name__ = kernel.__name__
    return body


def params():
    return pltpu.CompilerParams(vmem_limit_bytes=VMEM_LIMIT)


def grid_params():
    return pltpu.CompilerParams(dimension_semantics=("arbitrary",), vmem_limit_bytes=VMEM_LIMIT)


def ring(axis, step):
    count = lax.axis_size(axis)
    return [(i, (i + step) % count) for i in range(count)]


def turn_exchange(blocks, axis, against=False):
    count = len(blocks)
    out = [blocks[0]]
    for d in range(1, count):
        block = blocks[d]
        if against and 2 * d == count:
            for _ in range(d):
                block = lax.ppermute(block, axis, ring(axis, -1))
        else:
            block = lax.ppermute(block, axis, ring(axis, d))
        out.append(block)
    return out


def from_near(x, axis):
    return lax.ppermute(x, axis, ring(axis, 1)), lax.ppermute(x, axis, ring(axis, -1))


def from_far(pairs, axis):
    low = [before[: before.shape[0] // 2] for before, _ in pairs]
    high = [after[after.shape[0] // 2 :] for _, after in pairs]
    if len(pairs) == 1:
        low, high = low[0], high[0]
    else:
        low, high = jnp.concatenate(low, axis=0), jnp.concatenate(high, axis=0)
    return lax.ppermute(low, axis, ring(axis, 1)), lax.ppermute(high, axis, ring(axis, -1))


def exchange(x, axis):
    return lax.all_to_all(x, axis, split_axis=0, concat_axis=0, tiled=True)


def on_device(
    query_vectors,
    attend_lookup_vectors,
    attend_content_vectors,
    forget_speed_dependent,
    amend_speed_dependent,
    result_switch_preactivation,
    feature_forget_baseline,
    amend_speed_baseline,
    sudden_forget_extra,
    group_scaling_factor,
    result_mapping_matrix,
    specialist_tokens_activations,
    specialist_scaling_factor,
    selected_specialists,
    selection_mixing_factors,
    dispatched_switch_matrix,
    dispatched_raising_matrix,
    dispatched_lowering_matrix,
    common_switch_matrix,
    common_raising_matrix,
    common_lowering_matrix,
):
    tok_rows, top_count = selected_specialists.shape
    model = specialist_tokens_activations.shape[1]
    experts = lax.axis_size("ep")
    tp_size = lax.axis_size("tp")
    cap = 3 * tok_rows * top_count // (2 * experts)
    slot_rows = cap * 4 // 3
    main = model * 3 // 4
    third = model // 4
    total = experts * slot_rows

    ff = dispatched_switch_matrix.shape[2]
    me = lax.axis_index("tp").astype(jnp.int32).reshape(1)
    place = lax.axis_index("ep").astype(jnp.int32).reshape(1)

    gate_own, up_own, down_own = (
        dispatched_switch_matrix[0],
        dispatched_raising_matrix[0],
        dispatched_lowering_matrix[0],
    )
    gate_near = from_near(gate_own, "tp")
    up_near = from_near(up_own, "tp")
    down_near = from_near(down_own, "tp")
    both_far = from_far((gate_near, up_near), "tp")
    down_far = from_far((down_near,), "tp")

    normed, outgoing, positions = pl.pallas_call(
        bind(dispatch_kernel, slot_rows, cap),
        out_shape=[
            jax.ShapeDtypeStruct((tok_rows, model), BF16),
            jax.ShapeDtypeStruct((total, main), BF16),
            jax.ShapeDtypeStruct((tok_rows, top_count), jnp.int32),
        ],
        compiler_params=params(),
        name="dispatch",
    )(specialist_tokens_activations, specialist_scaling_factor.reshape(1, -1), selected_specialists.T)

    normed_all = turn_exchange([normed] * tp_size, "tp")

    received = exchange(outgoing.reshape(experts, slot_rows, main), "ep").reshape(total, main)

    out_local, q2, own_state = run_mixer_local(
        query_vectors,
        attend_lookup_vectors,
        attend_content_vectors,
        forget_speed_dependent,
        amend_speed_dependent,
        sudden_forget_extra,
        feature_forget_baseline,
        amend_speed_baseline,
    )
    all_states = lax.all_gather(own_state, "ep")
    starts = run_chain(place, all_states)

    anywhere = pl.BlockSpec(memory_space=pl.ANY)
    in_vmem = pl.BlockSpec(memory_space=pltpu.MemorySpace.VMEM)
    near = tp_size - 1
    kept = experts * cap
    hidden, rows = pl.pallas_call(
        bind(near_kernel, slot_rows, cap),
        in_specs=[in_vmem] + [anywhere] * (2 * near),
        out_shape=[
            jax.ShapeDtypeStruct((kept, near * ff), BF16),
            jax.ShapeDtypeStruct((kept, model), BF16),
        ],
        scratch_shapes=[
            pltpu.VMEM((near, model, ff), BF16),
            pltpu.VMEM((near, model, ff), BF16),
            pltpu.SemaphoreType.DMA((2 * near,)),
        ],
        compiler_params=params(),
        name="near",
    )(received, gate_own, *gate_near, up_own, *up_near)
    downs = (down_own, *down_near, *down_far)
    returning = pl.pallas_call(
        bind(far_kernel, slot_rows, cap),
        in_specs=[anywhere] * (4 + len(downs)),
        out_shape=jax.ShapeDtypeStruct((total, main), BF16),
        scratch_shapes=[
            pltpu.VMEM((kept, model), BF16),
            pltpu.VMEM((kept, tp_size * ff), BF16),
            pltpu.VMEM((model, ff), BF16),
            pltpu.VMEM((model, ff), BF16),
            pltpu.VMEM((tp_size * ff, model), BF16),
            pltpu.VMEM((kept, third), BF16),
            pltpu.SemaphoreType.DMA((6 + len(downs),)),
        ],
        compiler_params=params(),
        name="far",
    )(rows, hidden, *both_far, *downs)
    expert_out = exchange(returning.reshape(experts, slot_rows, main), "ep").reshape(total, main)

    shared_part = pl.pallas_call(
        shared_kernel,
        out_shape=[jax.ShapeDtypeStruct((tok_rows, model), BF16)] * tp_size,
        compiler_params=params(),
        name="shared",
    )(
        *(normed_all[(tp_size - d) % tp_size] for d in range(tp_size)),
        common_switch_matrix,
        common_raising_matrix,
        common_lowering_matrix,
    )
    shared_blocks = turn_exchange(shared_part, "tp")

    mixed_part = run_mixer_final(
        me,
        out_local,
        q2,
        starts,
        result_switch_preactivation,
        group_scaling_factor,
        result_mapping_matrix,
        tp_size,
    )
    mixed_blocks = turn_exchange(mixed_part, "tp", against=True)
    mixed_sum = mixed_blocks[0].astype(F32)
    for block in mixed_blocks[1:]:
        mixed_sum = mixed_sum + block.astype(F32)
    attend_result_matrix = mixed_sum.astype(BF16)
    weights, base = pl.pallas_call(
        bind(prepare_kernel, slot_rows, cap),
        out_shape=[
            jax.ShapeDtypeStruct((6 * tok_rows, total), BF16),
            jax.ShapeDtypeStruct((tok_rows, model), F32),
        ],
        compiler_params=params(),
        name="prepare",
    )(positions, selection_mixing_factors, *shared_blocks)
    moe_out = pl.pallas_call(
        combine_kernel,
        in_specs=[in_vmem] * 3,
        out_shape=jax.ShapeDtypeStruct((tok_rows, model), BF16),
        compiler_params=params(),
        name="combine",
    )(expert_out, weights, base)
    return (attend_result_matrix, moe_out)


def solution(mesh):
    by_rows = P(("grp", "ep"), "tp")
    by_device = P(("grp", "ep", "tp"), None)
    placed = (
        by_rows,
        by_rows,
        by_rows,
        by_rows,
        by_rows,
        by_rows,
        P("tp"),
        P("tp"),
        by_rows,
        P("tp"),
        P("tp", None),
        by_device,
        P(),
        by_device,
        by_device,
        P("ep", None, "tp"),
        P("ep", None, "tp"),
        P("ep", "tp", None),
        P(None, "tp"),
        P(None, "tp"),
        P("tp", None),
    )
    return jax.shard_map(
        on_device, mesh=mesh, in_specs=placed, out_specs=(by_device, by_device), check_vma=False
    )
```

```python
import jax
import jax.numpy as jnp
from jax import lax
from jax.experimental import pallas as pl
from jax.experimental.pallas import tpu as pltpu
from jax.sharding import PartitionSpec as P


F32 = jnp.float32
BF16 = jnp.bfloat16
SPAN = 64
VMEM_LIMIT = 56 * 1024 * 1024
SMALL_LIMIT = 20 * 1024 * 1024


def mm(a, b):
    return lax.dot_general(a, b, (((1,), (0,)), ((), ())), preferred_element_type=F32)


def mm_nt(a, b):
    return lax.dot_general(a, b, (((1,), (1,)), ((), ())), preferred_element_type=F32)


def mm_tn(a, b):
    return lax.dot_general(a, b, (((0,), (0,)), ((), ())), preferred_element_type=F32)


def iota(shape, dim):
    return lax.broadcasted_iota(jnp.int32, shape, dim)


def split_two(x):
    hi = x.astype(BF16)
    lo = (x - hi.astype(F32)).astype(BF16)
    return hi, lo


def sigmoid(x):
    return 1.0 / (1.0 + jnp.exp(-x))


def mixer_local(q_ref, k_ref, v_ref, f_ref, a_ref, x_ref, fb_ref, ab_ref, out_ref, q2_ref, ex_ref, state_ref):
    tokens, width = q_ref.shape
    half = width // 2
    spans = tokens // SPAN
    pair = pl.program_id(0)
    lane = iota((SPAN, width), 1)
    row = iota((SPAN, width), 0)
    first = lane < half
    col = lane % half
    strict = row > col
    inclusive = row >= col
    eye = (row == col).astype(F32)
    tril = (iota((SPAN, SPAN), 0) >= iota((SPAN, SPAN), 1)).astype(BF16)
    ones_bd = ((iota((2 * width, width), 0) % width) // half == iota((2 * width, width), 1) // half).astype(BF16)
    levels = []
    size = 1
    while size < SPAN:
        levels.append(
            (row // (2 * size) == col // (2 * size)) & (row % (2 * size) >= size) & (col % (2 * size) < size)
        )
        size *= 2

    def bd(x):
        zero = jnp.zeros_like(x)
        return jnp.concatenate([jnp.where(first, x, zero), jnp.where(first, zero, x)], axis=0)

    heads = x_ref.shape[1]
    head_lane = iota((SPAN, heads), 1)
    fb = fb_ref[...]
    ab = ab_ref[...]

    def prepare(c):
        rows = pl.ds(pl.multiple_of(c * SPAN, SPAN), SPAN)
        extra = x_ref[rows, :]
        extra_a = jnp.sum(jnp.where(head_lane == 2 * pair, extra, 0.0), axis=1, keepdims=True)
        extra_b = jnp.sum(jnp.where(head_lane == 2 * pair + 1, extra, 0.0), axis=1, keepdims=True)
        decay = jnp.where(first, extra_a, extra_b) - jnp.exp(fb + f_ref[rows, :].astype(F32))
        hi = decay.astype(BF16)
        rest = decay - hi.astype(F32)
        mid = rest.astype(BF16)
        low = (rest - mid.astype(F32)).astype(BF16)
        sums = mm(tril, jnp.concatenate([hi, mid, low], axis=1))
        cum = sums[:, :width] + sums[:, width : 2 * width] + sums[:, 2 * width :]
        key = k_ref[rows, :].astype(F32)
        sq_hi, sq_lo = split_two(key * key)
        total = mm(jnp.concatenate([sq_hi, sq_lo], axis=1), ones_bd) + 1e-06
        inv = lax.rsqrt(total)
        unit = key * inv
        erase = unit * sigmoid(ab + a_ref[rows, :].astype(F32))
        scaled_value = v_ref[rows, :].astype(F32) * (total * inv)
        center = cum[SPAN // 2 : SPAN // 2 + 1, :]
        last = cum[SPAN - 1 : SPAN, :]
        left_erase = -unit * jnp.exp(cum - decay - center)
        left_read = q_ref[rows, :].astype(F32) * jnp.exp(cum - center)
        right = erase * jnp.exp(center - cum)
        pairs = mm_nt(jnp.concatenate([left_erase, left_read], axis=0).astype(BF16), bd(right.astype(BF16)))
        lower = jnp.where(strict, pairs[:SPAN], 0.0)
        read = jnp.where(inclusive, pairs[SPAN:], 0.0).astype(BF16)
        to_start = jnp.exp(center)
        rhs = jnp.concatenate(
            [bd(scaled_value.astype(BF16)), bd((left_erase * to_start).astype(BF16))], axis=1
        )
        read_start = left_read * to_start
        tail = (right * jnp.exp(last - center)).astype(BF16)
        return lower, read, rhs, read_start, tail, jnp.exp(last)

    state_ref[...] = jnp.concatenate([jnp.zeros((SPAN, width), F32), eye], axis=0)
    group = min(4, spans)

    @pl.loop(0, spans // group)
    def _(turn):
        start = turn * group
        state = state_ref[...]
        prepared = [prepare(start + j) for j in range(group)]
        inverse = [eye + jnp.where(levels[0], p[0], 0.0) for p in prepared]
        for level in levels[1:]:
            packed = [x.astype(BF16) for x in inverse]
            step = [
                mm(x, bd(jnp.where(level, p[0], 0.0).astype(BF16))).astype(BF16)
                for x, p in zip(packed, prepared)
            ]
            inverse = [x + mm(y, bd(xb)) for x, y, xb in zip(inverse, step, packed)]
        solved = [mm(x.astype(BF16), p[2]).astype(BF16) for x, p in zip(inverse, prepared)]
        outs = [
            mm(p[1], jnp.concatenate([bd(u[:, :width]), bd(u[:, width:])], axis=1))
            for u, p in zip(solved, prepared)
        ]
        grams = [mm_tn(u, p[4]) for u, p in zip(solved, prepared)]
        for j in range(group):
            rows = pl.ds(pl.multiple_of((start + j) * SPAN, SPAN), SPAN)
            out, gram, prep = outs[j], grams[j], prepared[j]
            reads = (out[:, width:] + prep[3]).astype(BF16)
            state_b = state.astype(BF16)
            both = mm_nt(reads, jnp.concatenate([bd(state_b[:SPAN]), bd(state_b[SPAN:])], axis=0))
            out_ref[rows, :] = out[:, :width] + both[:, :width]
            q2_ref[rows, :] = both[:, width:].astype(BF16)
            add = jnp.where(first, gram[:SPAN], gram[SPAN : 2 * SPAN])
            trans = jnp.concatenate(
                [
                    jnp.where(first, gram[2 * SPAN : 3 * SPAN], 0.0),
                    jnp.where(first, 0.0, gram[3 * SPAN :]),
                ],
                axis=0,
            ).astype(BF16)
            state = state * prep[5] + mm(state_b, trans)
            state = jnp.concatenate([state[:SPAN] + add, state[SPAN:]], axis=0)
        state_ref[...] = state

    ex_ref[...] = state_ref[...].astype(BF16)


def run_mixer_local(q, k, v, f, a, extra, fb, ab):
    tokens, width = q.shape
    heads = extra.shape[1]
    head_size = width // heads
    pairs = heads // 2
    wide = 2 * head_size
    spec = pl.BlockSpec((tokens, wide), lambda i: (0, i))
    vec = pl.BlockSpec((1, wide), lambda i: (0, i))
    return pl.pallas_call(
        mixer_local,
        grid=(pairs,),
        in_specs=[spec] * 5 + [pl.BlockSpec((tokens, heads), lambda i: (0, 0)), vec, vec],
        out_specs=[spec, spec, pl.BlockSpec((wide, wide), lambda i: (i, 0))],
        out_shape=[
            jax.ShapeDtypeStruct((tokens, width), F32),
            jax.ShapeDtypeStruct((tokens, width), BF16),
            jax.ShapeDtypeStruct((pairs * wide, wide), BF16),
        ],
        scratch_shapes=[pltpu.VMEM((2 * SPAN, wide), F32)],
        compiler_params=pltpu.CompilerParams(
            dimension_semantics=("arbitrary",), vmem_limit_bytes=SMALL_LIMIT
        ),
        cost_estimate=pl.CostEstimate(
            flops=40_000_000_000, transcendentals=2_000_000, bytes_accessed=5_000_000
        ),
        name="mixer_local",
    )(q, k, v, f, a, extra, fb.reshape(1, -1), ab.reshape(1, -1))


def chain_kernel(me_ref, r_ref, o_ref, state_ref):
    rows, wide = r_ref.shape[1:]
    half = wide // 2
    pairs = rows // wide
    first = iota((half, wide), 1) < half
    state_ref[...] = jnp.zeros_like(state_ref)

    @pl.loop(0, r_ref.shape[0])
    def _(d):
        @pl.when(d < me_ref[0])
        def _():
            for p in range(pairs):
                own = slice(p * half, (p + 1) * half)
                added = r_ref[d, p * wide : p * wide + half, :].astype(F32)
                carried = r_ref[d, p * wide + half : (p + 1) * wide, :]
                zero = jnp.zeros_like(carried)
                carried = jnp.concatenate(
                    [jnp.where(first, carried, zero), jnp.where(first, zero, carried)], axis=0
                )
                state_ref[own, :] = mm(state_ref[own, :].astype(BF16), carried) + added

    o_ref[...] = state_ref[...].astype(BF16)


def run_chain(me, gathered):
    _, rows, wide = gathered.shape
    return pl.pallas_call(
        chain_kernel,
        grid_spec=pltpu.PrefetchScalarGridSpec(
            num_scalar_prefetch=1,
            grid=(1,),
            in_specs=[pl.BlockSpec(gathered.shape, lambda i, me_ref: (0, 0, 0))],
            out_specs=pl.BlockSpec((rows // 2, wide), lambda i, me_ref: (0, 0)),
            scratch_shapes=[pltpu.VMEM((rows // 2, wide), F32)],
        ),
        out_shape=jax.ShapeDtypeStruct((rows // 2, wide), BF16),
        compiler_params=grid_params(),
        cost_estimate=pl.CostEstimate(
            flops=3_000_000_000, transcendentals=0, bytes_accessed=4_000_000
        ),
        name="chain",
    )(me, gathered)


def mixer_final(me_ref, o_ref, q2_ref, s_ref, g_ref, gain_ref, w_ref, *outs):
    width = o_ref.shape[1]
    wide = s_ref.shape[1]
    half = wide // 2
    pairs = width // wide
    first = iota((half, wide), 1) < half
    ones_bd = ((iota((2 * wide, wide), 0) % wide) // half == iota((2 * wide, wide), 1) // half).astype(BF16)

    def head_mean(x):
        hi, lo = split_two(x)
        return mm(jnp.concatenate([hi, lo], axis=1), ones_bd) * (1.0 / half)

    pieces = []
    for p in range(pairs):
        cols = slice(p * wide, (p + 1) * wide)
        state = s_ref[p * half : (p + 1) * half, :]
        zero = jnp.zeros_like(state)
        both = jnp.concatenate([jnp.where(first, state, zero), jnp.where(first, zero, state)], axis=0)
        head_out = o_ref[:, cols] + mm_nt(q2_ref[:, cols], both)
        centered = head_out - head_mean(head_out)
        var = head_mean(centered * centered)
        gate = sigmoid(g_ref[:, cols].astype(F32))
        pieces.append((centered * lax.rsqrt(var + 0.00064) * gain_ref[:, cols] * gate).astype(BF16))
    mixed = jnp.concatenate(pieces, axis=1)
    result = mm(mixed, w_ref[...]).astype(BF16)
    for d, out_ref in enumerate(outs):

        @pl.when(pl.program_id(0) == d)
        def _(out_ref=out_ref):
            out_ref[...] = result


def run_mixer_final(me, out_local, q2, starts, gate, gain, mapping, blocks):
    tokens, width = out_local.shape
    model = mapping.shape[1]
    rows = tokens // blocks

    def turned(i, me_ref):
        return ((me_ref[0] + i) % blocks, 0)

    spec = pl.BlockSpec((rows, width), turned)
    return pl.pallas_call(
        mixer_final,
        grid_spec=pltpu.PrefetchScalarGridSpec(
            num_scalar_prefetch=1,
            grid=(blocks,),
            in_specs=[
                spec,
                spec,
                pl.BlockSpec(starts.shape, lambda i, me_ref: (0, 0)),
                spec,
                pl.BlockSpec((1, width), lambda i, me_ref: (0, 0)),
                pl.BlockSpec((width, model), lambda i, me_ref: (0, 0)),
            ],
            out_specs=[pl.BlockSpec((rows, model), lambda i, me_ref: (0, 0))] * blocks,
        ),
        out_shape=[jax.ShapeDtypeStruct((rows, model), BF16)] * blocks,
        compiler_params=grid_params(),
        cost_estimate=pl.CostEstimate(
            flops=6_000_000_000, transcendentals=1_000_000, bytes_accessed=8_000_000
        ),
        name="mixer_final",
    )(me, out_local, q2, starts, gate, gain.reshape(1, -1), mapping)


def picks(size, slot_rows, cap):
    kept = size // slot_rows * cap
    r = iota((kept, 1), 0)
    block = r // cap
    s = r - block * cap
    c = iota((kept, size), 1)
    at_tail = c == block * slot_rows + cap + s // 3
    return (c == block * slot_rows + s).astype(BF16), [
        (at_tail & (s % 3 == third)).astype(BF16) for third in range(3)
    ]


def dispatch_kernel(slot_rows, cap, t_ref, scale_ref, sel_ref, normed_ref, out_ref, pos_ref):
    rows, _ = t_ref.shape
    total = out_ref.shape[0]
    main = out_ref.shape[1]
    third = main // 3
    experts = total // slot_rows
    floats = t_ref[...].astype(F32)
    mean = jnp.mean(floats * floats, axis=1, keepdims=True)
    normed = (floats * lax.rsqrt(mean + 1e-06) * scale_ref[...]).astype(BF16)
    normed_ref[...] = normed
    named = sel_ref[...].astype(F32)
    named = jnp.concatenate([named] * (8 // named.shape[0]), axis=0).T.astype(jnp.int32)
    ids = [named[:, 0:1], named[:, 1:2]]
    expert = iota((rows, experts), 1)
    hot = [(i == expert).astype(F32) for i in ids]
    strict = (iota((rows, rows), 0) > iota((rows, rows), 1)).astype(BF16)
    before = mm(strict, (hot[0] + hot[1]).astype(BF16))
    slots = [jnp.sum(h * before, axis=1, keepdims=True).astype(jnp.int32) for h in hot]
    place = iota((rows, total), 1)
    pos = [i * slot_rows + s for i, s in zip(ids, slots)]
    tail = [i * slot_rows + cap + s // 3 for i, s in zip(ids, slots)]
    which = [s % 3 for s in slots]
    pos_ref[...] = jnp.concatenate(pos, axis=1)
    main_hot = ((place == pos[0]) | (place == pos[1])).astype(BF16)
    for b in range(3):
        tail_hot = (
            ((place == tail[0]) & (which[0] == b)) | ((place == tail[1]) & (which[1] == b))
        ).astype(BF16)
        hot2 = jnp.concatenate([main_hot, tail_hot], axis=0)
        data = jnp.concatenate([normed[:, b * third : (b + 1) * third], normed[:, main:]], axis=0)
        out_ref[:, b * third : (b + 1) * third] = mm_tn(hot2, data).astype(BF16)


def near_kernel(slot_rows, cap, r_ref, *refs):
    *others, h_ref, x_ref = refs
    count = len(others) // 2
    total, main = r_ref.shape
    third = main // 3
    ff = others[0].shape[1]
    size = min(256, total)
    kept = size // slot_rows * cap
    whole, tails = picks(size, slot_rows, cap)
    for i in range(total // size):
        rows = slice(i * kept, (i + 1) * kept)
        block = r_ref[i * size : (i + 1) * size, :]
        x_ref[rows, :main] = mm(whole, block).astype(BF16)
        acc = jnp.zeros((kept, third), F32)
        for b in range(3):
            acc = acc + mm(tails[b], block[:, b * third : (b + 1) * third])
        x_ref[rows, main:] = acc.astype(BF16)
    for k in range(count):
        gate = mm(x_ref[...], others[k][...])
        up = mm(x_ref[...], others[count + k][...])
        h_ref[:, k * ff : (k + 1) * ff] = (gate * sigmoid(gate) * up).astype(BF16)


def far_kernel(slot_rows, cap, x_ref, h_ref, gate_ref, up_ref, fa_ref, fb_ref, *refs):
    *downs, o_ref, f_ref, tail_ref = refs
    total, main = o_ref.shape
    third = main // 3
    half = fa_ref.shape[0] // 2
    ff = gate_ref.shape[1]
    size = min(256, total)
    kept = size // slot_rows * cap
    whole, tails = picks(size, slot_rows, cap)
    gate = mm(x_ref[...], gate_ref[...])
    up = mm(x_ref[...], up_ref[...])
    f_ref[:, :ff] = (gate * sigmoid(gate) * up).astype(BF16)
    low, high = x_ref[:, :half], x_ref[:, half:]
    gate = mm(low, fa_ref[:half]) + mm(high, fb_ref[:half])
    up = mm(low, fa_ref[half:]) + mm(high, fb_ref[half:])
    f_ref[:, ff:] = (gate * sigmoid(gate) * up).astype(BF16)

    def lower(cols):
        acc = None
        at = 0
        for d_ref in downs:
            count = d_ref.shape[0]
            if at < h_ref.shape[1]:
                h = h_ref[:, at : at + count]
            else:
                h = f_ref[:, at - h_ref.shape[1] : at - h_ref.shape[1] + count]
            part = mm(h, d_ref[:, cols])
            acc = part if acc is None else acc + part
            at += count
        return acc.astype(BF16)

    tail_ref[...] = lower(slice(main, main + third))
    for b in range(3):
        cols = slice(b * third, (b + 1) * third)
        y = lower(cols)
        spread = jnp.concatenate([whole, tails[b]], axis=0)
        for i in range(total // size):
            rows = slice(i * kept, (i + 1) * kept)
            both = jnp.concatenate([y[rows], tail_ref[rows, :]], axis=0)
            o_ref[i * size : (i + 1) * size, cols] = mm_tn(spread, both).astype(BF16)


def shared_kernel(*refs):
    count = len(refs) // 2 - 1
    rows_in, outs = refs[:count], refs[count + 3 :]
    g_ref, u_ref, d_ref = refs[count : count + 3]
    x = jnp.concatenate([ref[...] for ref in rows_in], axis=0)
    gate = mm(x, g_ref[...])
    up = mm(x, u_ref[...])
    hidden = (gate * sigmoid(gate) * up).astype(BF16)
    for d, o_ref in enumerate(outs):
        rows = o_ref.shape[0]
        o_ref[...] = mm(hidden[d * rows : (d + 1) * rows], d_ref[...]).astype(BF16)


def prepare_kernel(slot_rows, cap, pos_ref, mix_ref, *refs):
    *blocks, w_ref, base_ref = refs
    rows = pos_ref.shape[0]
    place = iota((rows, w_ref.shape[1]), 1)
    pos = [pos_ref[:, 0:1], pos_ref[:, 1:2]]
    mix = [mix_ref[:, 0:1], mix_ref[:, 1:2]]
    slots = [p % slot_rows for p in pos]
    tail = [p - s + cap + s // 3 for p, s in zip(pos, slots)]
    which = [s % 3 for s in slots]
    main = jnp.where(place == pos[0], mix[0], 0.0) + jnp.where(place == pos[1], mix[1], 0.0)
    main = main.astype(BF16)
    for b in range(3):
        w_ref[2 * b * rows : (2 * b + 1) * rows, :] = main
        w_ref[(2 * b + 1) * rows : (2 * b + 2) * rows, :] = (
            jnp.where((place == tail[0]) & (which[0] == b), mix[0], 0.0)
            + jnp.where((place == tail[1]) & (which[1] == b), mix[1], 0.0)
        ).astype(BF16)
    base = blocks[0][...].astype(F32)
    for block in blocks[1:]:
        base = base + block[...].astype(F32)
    base_ref[...] = base


def combine_kernel(z_ref, w_ref, base_ref, o_ref):
    main = z_ref.shape[1]
    rows = o_ref.shape[0]
    third = main // 3
    tail_sum = base_ref[:, main:]
    for b in range(3):
        cols = slice(b * third, (b + 1) * third)
        both = mm(w_ref[2 * b * rows : 2 * (b + 1) * rows, :], z_ref[:, cols])
        o_ref[:, cols] = (base_ref[:, cols] + both[:rows]).astype(BF16)
        tail_sum = tail_sum + both[rows:]
    o_ref[:, main:] = tail_sum.astype(BF16)


def bind(kernel, *static):
    def body(*refs):
        kernel(*static, *refs)

    body.__name__ = kernel.__name__
    return body


def params(limit=VMEM_LIMIT):
    return pltpu.CompilerParams(vmem_limit_bytes=limit)


def grid_params():
    return pltpu.CompilerParams(dimension_semantics=("arbitrary",), vmem_limit_bytes=VMEM_LIMIT)


def ring(axis, step):
    count = lax.axis_size(axis)
    return [(i, (i + step) % count) for i in range(count)]


def turn_exchange(blocks, axis):
    return [blocks[0]] + [lax.ppermute(blocks[d], axis, ring(axis, d)) for d in range(1, len(blocks))]


def from_near(x, axis):
    return lax.ppermute(x, axis, ring(axis, 1)), lax.ppermute(x, axis, ring(axis, -1))


def from_far(pairs, axis):
    low = [before[: before.shape[0] // 2] for before, _ in pairs]
    high = [after[after.shape[0] // 2 :] for _, after in pairs]
    if len(pairs) == 1:
        low, high = low[0], high[0]
    else:
        low, high = jnp.concatenate(low, axis=0), jnp.concatenate(high, axis=0)
    return lax.ppermute(low, axis, ring(axis, 1)), lax.ppermute(high, axis, ring(axis, -1))


def exchange(x, axis):
    return lax.all_to_all(x, axis, split_axis=0, concat_axis=0, tiled=True)


def on_device(
    query_vectors,
    attend_lookup_vectors,
    attend_content_vectors,
    forget_speed_dependent,
    amend_speed_dependent,
    result_switch_preactivation,
    feature_forget_baseline,
    amend_speed_baseline,
    sudden_forget_extra,
    group_scaling_factor,
    result_mapping_matrix,
    specialist_tokens_activations,
    specialist_scaling_factor,
    selected_specialists,
    selection_mixing_factors,
    dispatched_switch_matrix,
    dispatched_raising_matrix,
    dispatched_lowering_matrix,
    common_switch_matrix,
    common_raising_matrix,
    common_lowering_matrix,
):
    tok_rows, top_count = selected_specialists.shape
    model = specialist_tokens_activations.shape[1]
    experts = lax.axis_size("ep")
    tp_size = lax.axis_size("tp")
    cap = 3 * tok_rows * top_count // (2 * experts)
    slot_rows = cap * 4 // 3
    main = model * 3 // 4
    third = model // 4
    total = experts * slot_rows

    ff = dispatched_switch_matrix.shape[2]
    me = lax.axis_index("tp").astype(jnp.int32).reshape(1)
    place = lax.axis_index("ep").astype(jnp.int32).reshape(1)

    gate_own, up_own, down_own = (
        dispatched_switch_matrix[0],
        dispatched_raising_matrix[0],
        dispatched_lowering_matrix[0],
    )
    gate_near = from_near(gate_own, "tp")
    up_near = from_near(up_own, "tp")
    down_near = from_near(down_own, "tp")
    both_far = from_far((gate_near, up_near), "tp")
    down_far = from_far((down_near,), "tp")

    normed, outgoing, positions = pl.pallas_call(
        bind(dispatch_kernel, slot_rows, cap),
        out_shape=[
            jax.ShapeDtypeStruct((tok_rows, model), BF16),
            jax.ShapeDtypeStruct((total, main), BF16),
            jax.ShapeDtypeStruct((tok_rows, top_count), jnp.int32),
        ],
        compiler_params=params(),
        name="dispatch",
    )(specialist_tokens_activations, specialist_scaling_factor.reshape(1, -1), selected_specialists.T)

    normed_near = from_near(normed, "tp")
    normed_far = from_far((normed_near,), "tp")

    received = exchange(outgoing.reshape(experts, slot_rows, main), "ep").reshape(total, main)

    out_local, q2, own_state = run_mixer_local(
        query_vectors,
        attend_lookup_vectors,
        attend_content_vectors,
        forget_speed_dependent,
        amend_speed_dependent,
        sudden_forget_extra,
        feature_forget_baseline,
        amend_speed_baseline,
    )
    all_states = lax.all_gather(own_state, "ep")
    starts = run_chain(place, all_states)

    in_vmem = pl.BlockSpec(memory_space=pltpu.MemorySpace.VMEM)
    kept = experts * cap
    hidden, rows = pl.pallas_call(
        bind(near_kernel, slot_rows, cap),
        in_specs=[in_vmem] * 5,
        out_specs=[in_vmem] * 2,
        out_shape=[
            jax.ShapeDtypeStruct((kept, 2 * ff), BF16),
            jax.ShapeDtypeStruct((kept, model), BF16),
        ],
        compiler_params=params(SMALL_LIMIT),
        name="near",
    )(received, *gate_near, *up_near)
    downs = (*down_near, down_own, *down_far)
    returning = pl.pallas_call(
        bind(far_kernel, slot_rows, cap),
        in_specs=[in_vmem] * (6 + len(downs)),
        out_shape=jax.ShapeDtypeStruct((total, main), BF16),
        scratch_shapes=[pltpu.VMEM((kept, 2 * ff), BF16), pltpu.VMEM((kept, third), BF16)],
        compiler_params=params(SMALL_LIMIT),
        name="far",
    )(rows, hidden, gate_own, up_own, *both_far, *downs)
    expert_out = exchange(returning.reshape(experts, slot_rows, main), "ep").reshape(total, main)

    shared_part = pl.pallas_call(
        shared_kernel,
        out_shape=[jax.ShapeDtypeStruct((tok_rows, model), BF16)] * tp_size,
        compiler_params=params(),
        name="shared",
    )(
        normed,
        normed_near[1],
        *normed_far,
        normed_near[0],
        common_switch_matrix,
        common_raising_matrix,
        common_lowering_matrix,
    )
    shared_blocks = turn_exchange(shared_part, "tp")

    mixed_part = run_mixer_final(
        me,
        out_local,
        q2,
        starts,
        result_switch_preactivation,
        group_scaling_factor,
        result_mapping_matrix,
        tp_size,
    )
    mixed_blocks = turn_exchange(mixed_part, "tp")
    mixed_sum = mixed_blocks[0].astype(F32)
    for block in mixed_blocks[1:]:
        mixed_sum = mixed_sum + block.astype(F32)
    attend_result_matrix = mixed_sum.astype(BF16)
    weights, base = pl.pallas_call(
        bind(prepare_kernel, slot_rows, cap),
        out_shape=[
            jax.ShapeDtypeStruct((6 * tok_rows, total), BF16),
            jax.ShapeDtypeStruct((tok_rows, model), F32),
        ],
        compiler_params=params(),
        name="prepare",
    )(positions, selection_mixing_factors, *shared_blocks)
    moe_out = pl.pallas_call(
        combine_kernel,
        in_specs=[in_vmem] * 3,
        out_shape=jax.ShapeDtypeStruct((tok_rows, model), BF16),
        compiler_params=params(),
        name="combine",
    )(expert_out, weights, base)
    return (attend_result_matrix, moe_out)


def solution(mesh):
    by_rows = P(("grp", "ep"), "tp")
    by_device = P(("grp", "ep", "tp"), None)
    placed = (
        by_rows,
        by_rows,
        by_rows,
        by_rows,
        by_rows,
        by_rows,
        P("tp"),
        P("tp"),
        by_rows,
        P("tp"),
        P("tp", None),
        by_device,
        P(),
        by_device,
        by_device,
        P("ep", None, "tp"),
        P("ep", None, "tp"),
        P("ep", "tp", None),
        P(None, "tp"),
        P(None, "tp"),
        P("tp", None),
    )
    return jax.shard_map(
        on_device, mesh=mesh, in_specs=placed, out_specs=(by_device, by_device), check_vma=False
    )
```

```python
import jax
import jax.numpy as jnp
from jax import lax
from jax.experimental import pallas as pl
from jax.experimental.pallas import tpu as pltpu
from jax.sharding import PartitionSpec as P


F32 = jnp.float32
BF16 = jnp.bfloat16
SPAN = 64
VMEM_LIMIT = 56 * 1024 * 1024
SMALL_LIMIT = 20 * 1024 * 1024


def mm(a, b):
    return lax.dot_general(a, b, (((1,), (0,)), ((), ())), preferred_element_type=F32)


def mm_nt(a, b):
    return lax.dot_general(a, b, (((1,), (1,)), ((), ())), preferred_element_type=F32)


def mm_tn(a, b):
    return lax.dot_general(a, b, (((0,), (0,)), ((), ())), preferred_element_type=F32)


def iota(shape, dim):
    return lax.broadcasted_iota(jnp.int32, shape, dim)


def split_two(x):
    hi = x.astype(BF16)
    lo = (x - hi.astype(F32)).astype(BF16)
    return hi, lo


def sigmoid(x):
    return 1.0 / (1.0 + jnp.exp(-x))


def mixer_local(q_ref, k_ref, v_ref, f_ref, a_ref, x_ref, fb_ref, ab_ref, out_ref, q2_ref, ex_ref, state_ref):
    tokens, width = q_ref.shape
    half = width // 2
    spans = tokens // SPAN
    pair = pl.program_id(0)
    lane = iota((SPAN, width), 1)
    row = iota((SPAN, width), 0)
    first = lane < half
    col = lane % half
    strict = row > col
    inclusive = row >= col
    eye = (row == col).astype(F32)
    tril = (iota((SPAN, SPAN), 0) >= iota((SPAN, SPAN), 1)).astype(BF16)
    ones_bd = ((iota((2 * width, width), 0) % width) // half == iota((2 * width, width), 1) // half).astype(BF16)
    levels = []
    size = 1
    while size < SPAN:
        levels.append(
            (row // (2 * size) == col // (2 * size)) & (row % (2 * size) >= size) & (col % (2 * size) < size)
        )
        size *= 2

    def bd(x):
        zero = jnp.zeros_like(x)
        return jnp.concatenate([jnp.where(first, x, zero), jnp.where(first, zero, x)], axis=0)

    heads = x_ref.shape[1]
    head_lane = iota((SPAN, heads), 1)
    fb = fb_ref[...]
    ab = ab_ref[...]

    def prepare(c):
        rows = pl.ds(pl.multiple_of(c * SPAN, SPAN), SPAN)
        extra = x_ref[rows, :]
        extra_a = jnp.sum(jnp.where(head_lane == 2 * pair, extra, 0.0), axis=1, keepdims=True)
        extra_b = jnp.sum(jnp.where(head_lane == 2 * pair + 1, extra, 0.0), axis=1, keepdims=True)
        decay = jnp.where(first, extra_a, extra_b) - jnp.exp(fb + f_ref[rows, :].astype(F32))
        hi = decay.astype(BF16)
        rest = decay - hi.astype(F32)
        mid = rest.astype(BF16)
        low = (rest - mid.astype(F32)).astype(BF16)
        sums = mm(tril, jnp.concatenate([hi, mid, low], axis=1))
        cum = sums[:, :width] + sums[:, width : 2 * width] + sums[:, 2 * width :]
        key = k_ref[rows, :].astype(F32)
        sq_hi, sq_lo = split_two(key * key)
        total = mm(jnp.concatenate([sq_hi, sq_lo], axis=1), ones_bd) + 1e-06
        inv = lax.rsqrt(total)
        unit = key * inv
        erase = unit * sigmoid(ab + a_ref[rows, :].astype(F32))
        scaled_value = v_ref[rows, :].astype(F32) * (total * inv)
        center = cum[SPAN // 2 : SPAN // 2 + 1, :]
        last = cum[SPAN - 1 : SPAN, :]
        left_erase = -unit * jnp.exp(cum - decay - center)
        left_read = q_ref[rows, :].astype(F32) * jnp.exp(cum - center)
        right = erase * jnp.exp(center - cum)
        pairs = mm_nt(jnp.concatenate([left_erase, left_read], axis=0).astype(BF16), bd(right.astype(BF16)))
        lower = jnp.where(strict, pairs[:SPAN], 0.0)
        read = jnp.where(inclusive, pairs[SPAN:], 0.0).astype(BF16)
        to_start = jnp.exp(center)
        rhs = jnp.concatenate(
            [bd(scaled_value.astype(BF16)), bd((left_erase * to_start).astype(BF16))], axis=1
        )
        read_start = left_read * to_start
        tail = (right * jnp.exp(last - center)).astype(BF16)
        return lower, read, rhs, read_start, tail, jnp.exp(last)

    state_ref[...] = jnp.concatenate([jnp.zeros((SPAN, width), F32), eye], axis=0)
    group = min(4, spans)

    @pl.loop(0, spans // group)
    def _(turn):
        start = turn * group
        state = state_ref[...]
        prepared = [prepare(start + j) for j in range(group)]
        inverse = [eye + jnp.where(levels[0], p[0], 0.0) for p in prepared]
        for level in levels[1:]:
            packed = [x.astype(BF16) for x in inverse]
            step = [
                mm(x, bd(jnp.where(level, p[0], 0.0).astype(BF16))).astype(BF16)
                for x, p in zip(packed, prepared)
            ]
            inverse = [x + mm(y, bd(xb)) for x, y, xb in zip(inverse, step, packed)]
        solved = [mm(x.astype(BF16), p[2]).astype(BF16) for x, p in zip(inverse, prepared)]
        outs = [
            mm(p[1], jnp.concatenate([bd(u[:, :width]), bd(u[:, width:])], axis=1))
            for u, p in zip(solved, prepared)
        ]
        grams = [mm_tn(u, p[4]) for u, p in zip(solved, prepared)]
        for j in range(group):
            rows = pl.ds(pl.multiple_of((start + j) * SPAN, SPAN), SPAN)
            out, gram, prep = outs[j], grams[j], prepared[j]
            reads = (out[:, width:] + prep[3]).astype(BF16)
            state_b = state.astype(BF16)
            both = mm_nt(reads, jnp.concatenate([bd(state_b[:SPAN]), bd(state_b[SPAN:])], axis=0))
            out_ref[rows, :] = out[:, :width] + both[:, :width]
            q2_ref[rows, :] = both[:, width:].astype(BF16)
            add = jnp.where(first, gram[:SPAN], gram[SPAN : 2 * SPAN])
            trans = jnp.concatenate(
                [
                    jnp.where(first, gram[2 * SPAN : 3 * SPAN], 0.0),
                    jnp.where(first, 0.0, gram[3 * SPAN :]),
                ],
                axis=0,
            ).astype(BF16)
            state = state * prep[5] + mm(state_b, trans)
            state = jnp.concatenate([state[:SPAN] + add, state[SPAN:]], axis=0)
        state_ref[...] = state

    ex_ref[...] = state_ref[...].astype(BF16)


def run_mixer_local(q, k, v, f, a, extra, fb, ab):
    tokens, width = q.shape
    heads = extra.shape[1]
    head_size = width // heads
    pairs = heads // 2
    wide = 2 * head_size
    spec = pl.BlockSpec((tokens, wide), lambda i: (0, i))
    vec = pl.BlockSpec((1, wide), lambda i: (0, i))
    return pl.pallas_call(
        mixer_local,
        grid=(pairs,),
        in_specs=[spec] * 5 + [pl.BlockSpec((tokens, heads), lambda i: (0, 0)), vec, vec],
        out_specs=[spec, spec, pl.BlockSpec((wide, wide), lambda i: (i, 0))],
        out_shape=[
            jax.ShapeDtypeStruct((tokens, width), F32),
            jax.ShapeDtypeStruct((tokens, width), BF16),
            jax.ShapeDtypeStruct((pairs * wide, wide), BF16),
        ],
        scratch_shapes=[pltpu.VMEM((2 * SPAN, wide), F32)],
        compiler_params=pltpu.CompilerParams(
            dimension_semantics=("arbitrary",), vmem_limit_bytes=SMALL_LIMIT
        ),
        cost_estimate=pl.CostEstimate(
            flops=40_000_000_000, transcendentals=2_000_000, bytes_accessed=5_000_000
        ),
        name="mixer_local",
    )(q, k, v, f, a, extra, fb.reshape(1, -1), ab.reshape(1, -1))


def chain_kernel(me_ref, r_ref, o_ref, state_ref):
    rows, wide = r_ref.shape[1:]
    half = wide // 2
    pairs = rows // wide
    first = iota((half, wide), 1) < half
    state_ref[...] = jnp.zeros_like(state_ref)

    @pl.loop(0, r_ref.shape[0])
    def _(d):
        @pl.when(d < me_ref[0])
        def _():
            for p in range(pairs):
                own = slice(p * half, (p + 1) * half)
                added = r_ref[d, p * wide : p * wide + half, :].astype(F32)
                carried = r_ref[d, p * wide + half : (p + 1) * wide, :]
                zero = jnp.zeros_like(carried)
                carried = jnp.concatenate(
                    [jnp.where(first, carried, zero), jnp.where(first, zero, carried)], axis=0
                )
                state_ref[own, :] = mm(state_ref[own, :].astype(BF16), carried) + added

    o_ref[...] = state_ref[...].astype(BF16)


def run_chain(me, gathered):
    _, rows, wide = gathered.shape
    return pl.pallas_call(
        chain_kernel,
        grid_spec=pltpu.PrefetchScalarGridSpec(
            num_scalar_prefetch=1,
            grid=(1,),
            in_specs=[pl.BlockSpec(gathered.shape, lambda i, me_ref: (0, 0, 0))],
            out_specs=pl.BlockSpec((rows // 2, wide), lambda i, me_ref: (0, 0)),
            scratch_shapes=[pltpu.VMEM((rows // 2, wide), F32)],
        ),
        out_shape=jax.ShapeDtypeStruct((rows // 2, wide), BF16),
        compiler_params=grid_params(),
        cost_estimate=pl.CostEstimate(
            flops=3_000_000_000, transcendentals=0, bytes_accessed=4_000_000
        ),
        name="chain",
    )(me, gathered)


def mixer_final(me_ref, o_ref, q2_ref, s_ref, g_ref, gain_ref, w_ref, *outs):
    width = o_ref.shape[1]
    wide = s_ref.shape[1]
    half = wide // 2
    pairs = width // wide
    first = iota((half, wide), 1) < half
    ones_bd = ((iota((2 * wide, wide), 0) % wide) // half == iota((2 * wide, wide), 1) // half).astype(BF16)

    def head_mean(x):
        hi, lo = split_two(x)
        return mm(jnp.concatenate([hi, lo], axis=1), ones_bd) * (1.0 / half)

    pieces = []
    for p in range(pairs):
        cols = slice(p * wide, (p + 1) * wide)
        state = s_ref[p * half : (p + 1) * half, :]
        zero = jnp.zeros_like(state)
        both = jnp.concatenate([jnp.where(first, state, zero), jnp.where(first, zero, state)], axis=0)
        head_out = o_ref[:, cols] + mm_nt(q2_ref[:, cols], both)
        centered = head_out - head_mean(head_out)
        var = head_mean(centered * centered)
        gate = sigmoid(g_ref[:, cols].astype(F32))
        pieces.append((centered * lax.rsqrt(var + 0.00064) * gain_ref[:, cols] * gate).astype(BF16))
    mixed = jnp.concatenate(pieces, axis=1)
    result = mm(mixed, w_ref[...]).astype(BF16)
    for d, out_ref in enumerate(outs):

        @pl.when(pl.program_id(0) == d)
        def _(out_ref=out_ref):
            out_ref[...] = result


def run_mixer_final(me, out_local, q2, starts, gate, gain, mapping, blocks):
    tokens, width = out_local.shape
    model = mapping.shape[1]
    rows = tokens // blocks

    def turned(i, me_ref):
        return ((me_ref[0] + i) % blocks, 0)

    spec = pl.BlockSpec((rows, width), turned)
    return pl.pallas_call(
        mixer_final,
        grid_spec=pltpu.PrefetchScalarGridSpec(
            num_scalar_prefetch=1,
            grid=(blocks,),
            in_specs=[
                spec,
                spec,
                pl.BlockSpec(starts.shape, lambda i, me_ref: (0, 0)),
                spec,
                pl.BlockSpec((1, width), lambda i, me_ref: (0, 0)),
                pl.BlockSpec((width, model), lambda i, me_ref: (0, 0)),
            ],
            out_specs=[pl.BlockSpec((rows, model), lambda i, me_ref: (0, 0))] * blocks,
        ),
        out_shape=[jax.ShapeDtypeStruct((rows, model), BF16)] * blocks,
        compiler_params=grid_params(),
        cost_estimate=pl.CostEstimate(
            flops=6_000_000_000, transcendentals=1_000_000, bytes_accessed=8_000_000
        ),
        name="mixer_final",
    )(me, out_local, q2, starts, gate, gain.reshape(1, -1), mapping)


def picks(size, slot_rows, cap):
    kept = size // slot_rows * cap
    r = iota((kept, 1), 0)
    block = r // cap
    s = r - block * cap
    c = iota((kept, size), 1)
    at_tail = c == block * slot_rows + cap + s // 3
    return (c == block * slot_rows + s).astype(BF16), [
        (at_tail & (s % 3 == third)).astype(BF16) for third in range(3)
    ]


def dispatch_kernel(slot_rows, cap, t_ref, scale_ref, sel_ref, normed_ref, out_ref, pos_ref):
    rows, _ = t_ref.shape
    total = out_ref.shape[0]
    main = out_ref.shape[1]
    third = main // 3
    experts = total // slot_rows
    floats = t_ref[...].astype(F32)
    mean = jnp.mean(floats * floats, axis=1, keepdims=True)
    normed = (floats * lax.rsqrt(mean + 1e-06) * scale_ref[...]).astype(BF16)
    normed_ref[...] = normed
    named = sel_ref[...].astype(F32)
    named = jnp.concatenate([named] * (8 // named.shape[0]), axis=0).T.astype(jnp.int32)
    ids = [named[:, 0:1], named[:, 1:2]]
    expert = iota((rows, experts), 1)
    hot = [(i == expert).astype(F32) for i in ids]
    strict = (iota((rows, rows), 0) > iota((rows, rows), 1)).astype(BF16)
    before = mm(strict, (hot[0] + hot[1]).astype(BF16))
    slots = [jnp.sum(h * before, axis=1, keepdims=True).astype(jnp.int32) for h in hot]
    place = iota((rows, total), 1)
    pos = [i * slot_rows + s for i, s in zip(ids, slots)]
    tail = [i * slot_rows + cap + s // 3 for i, s in zip(ids, slots)]
    which = [s % 3 for s in slots]
    pos_ref[...] = jnp.concatenate(pos, axis=1)
    main_hot = ((place == pos[0]) | (place == pos[1])).astype(BF16)
    for b in range(3):
        tail_hot = (
            ((place == tail[0]) & (which[0] == b)) | ((place == tail[1]) & (which[1] == b))
        ).astype(BF16)
        hot2 = jnp.concatenate([main_hot, tail_hot], axis=0)
        data = jnp.concatenate([normed[:, b * third : (b + 1) * third], normed[:, main:]], axis=0)
        out_ref[:, b * third : (b + 1) * third] = mm_tn(hot2, data).astype(BF16)


def near_kernel(slot_rows, cap, r_ref, *refs):
    *weights, x_ref, y_ref, h_ref = refs
    count = len(weights) // 3
    gates, ups, downs = weights[:count], weights[count : 2 * count], weights[2 * count :]
    total, main = r_ref.shape
    third = main // 3
    ff = gates[0].shape[1]
    size = min(256, total)
    kept = size // slot_rows * cap
    whole, tails = picks(size, slot_rows, cap)
    for i in range(total // size):
        rows = slice(i * kept, (i + 1) * kept)
        block = r_ref[i * size : (i + 1) * size, :]
        x_ref[rows, :main] = mm(whole, block).astype(BF16)
        acc = jnp.zeros((kept, third), F32)
        for b in range(3):
            acc = acc + mm(tails[b], block[:, b * third : (b + 1) * third])
        x_ref[rows, main:] = acc.astype(BF16)
    for k in range(count):
        gate = mm(x_ref[...], gates[k][...])
        up = mm(x_ref[...], ups[k][...])
        h_ref[:, k * ff : (k + 1) * ff] = (gate * sigmoid(gate) * up).astype(BF16)
    for b in range(4):
        cols = slice(b * third, (b + 1) * third)
        acc = mm(h_ref[:, :ff], downs[0][:, cols])
        for k in range(1, count):
            acc = acc + mm(h_ref[:, k * ff : (k + 1) * ff], downs[k][:, cols])
        y_ref[:, cols] = acc


def far_kernel(slot_rows, cap, x_ref, y_ref, fa_ref, fb_ref, da_ref, db_ref, o_ref, f_ref, tail_ref):
    total, main = o_ref.shape
    third = main // 3
    half = fa_ref.shape[0] // 2
    low_ff = da_ref.shape[0]
    size = min(256, total)
    kept = size // slot_rows * cap
    whole, tails = picks(size, slot_rows, cap)
    low, high = x_ref[:, :half], x_ref[:, half:]
    gate = mm(low, fa_ref[:half]) + mm(high, fb_ref[:half])
    up = mm(low, fa_ref[half:]) + mm(high, fb_ref[half:])
    f_ref[...] = (gate * sigmoid(gate) * up).astype(BF16)

    def lower(cols):
        far = mm(f_ref[:, :low_ff], da_ref[:, cols]) + mm(f_ref[:, low_ff:], db_ref[:, cols])
        return (y_ref[:, cols] + far).astype(BF16)

    tail_ref[...] = lower(slice(main, main + third))
    for b in range(3):
        cols = slice(b * third, (b + 1) * third)
        y = lower(cols)
        spread = jnp.concatenate([whole, tails[b]], axis=0)
        for i in range(total // size):
            rows = slice(i * kept, (i + 1) * kept)
            both = jnp.concatenate([y[rows], tail_ref[rows, :]], axis=0)
            o_ref[i * size : (i + 1) * size, cols] = mm_tn(spread, both).astype(BF16)


def shared_kernel(*refs):
    count = len(refs) // 2 - 1
    rows_in, outs = refs[:count], refs[count + 3 :]
    g_ref, u_ref, d_ref = refs[count : count + 3]
    x = jnp.concatenate([ref[...] for ref in rows_in], axis=0)
    gate = mm(x, g_ref[...])
    up = mm(x, u_ref[...])
    hidden = (gate * sigmoid(gate) * up).astype(BF16)
    for d, o_ref in enumerate(outs):
        rows = o_ref.shape[0]
        o_ref[...] = mm(hidden[d * rows : (d + 1) * rows], d_ref[...]).astype(BF16)


def prepare_kernel(slot_rows, cap, pos_ref, mix_ref, *refs):
    *blocks, w_ref, base_ref = refs
    rows = pos_ref.shape[0]
    place = iota((rows, w_ref.shape[1]), 1)
    pos = [pos_ref[:, 0:1], pos_ref[:, 1:2]]
    mix = [mix_ref[:, 0:1], mix_ref[:, 1:2]]
    slots = [p % slot_rows for p in pos]
    tail = [p - s + cap + s // 3 for p, s in zip(pos, slots)]
    which = [s % 3 for s in slots]
    main = jnp.where(place == pos[0], mix[0], 0.0) + jnp.where(place == pos[1], mix[1], 0.0)
    main = main.astype(BF16)
    for b in range(3):
        w_ref[2 * b * rows : (2 * b + 1) * rows, :] = main
        w_ref[(2 * b + 1) * rows : (2 * b + 2) * rows, :] = (
            jnp.where((place == tail[0]) & (which[0] == b), mix[0], 0.0)
            + jnp.where((place == tail[1]) & (which[1] == b), mix[1], 0.0)
        ).astype(BF16)
    base = blocks[0][...].astype(F32)
    for block in blocks[1:]:
        base = base + block[...].astype(F32)
    base_ref[...] = base


def combine_kernel(z_ref, w_ref, base_ref, o_ref):
    main = z_ref.shape[1]
    rows = o_ref.shape[0]
    third = main // 3
    tail_sum = base_ref[:, main:]
    for b in range(3):
        cols = slice(b * third, (b + 1) * third)
        both = mm(w_ref[2 * b * rows : 2 * (b + 1) * rows, :], z_ref[:, cols])
        o_ref[:, cols] = (base_ref[:, cols] + both[:rows]).astype(BF16)
        tail_sum = tail_sum + both[rows:]
    o_ref[:, main:] = tail_sum.astype(BF16)


def bind(kernel, *static):
    def body(*refs):
        kernel(*static, *refs)

    body.__name__ = kernel.__name__
    return body


def params(limit=VMEM_LIMIT):
    return pltpu.CompilerParams(vmem_limit_bytes=limit)


def grid_params():
    return pltpu.CompilerParams(dimension_semantics=("arbitrary",), vmem_limit_bytes=VMEM_LIMIT)


def ring(axis, step):
    count = lax.axis_size(axis)
    return [(i, (i + step) % count) for i in range(count)]


def turn_exchange(blocks, axis):
    return [blocks[0]] + [lax.ppermute(blocks[d], axis, ring(axis, d)) for d in range(1, len(blocks))]


def from_near(x, axis):
    return lax.ppermute(x, axis, ring(axis, 1)), lax.ppermute(x, axis, ring(axis, -1))


def from_far(pairs, axis):
    low = [before[: before.shape[0] // 2] for before, _ in pairs]
    high = [after[after.shape[0] // 2 :] for _, after in pairs]
    if len(pairs) == 1:
        low, high = low[0], high[0]
    else:
        low, high = jnp.concatenate(low, axis=0), jnp.concatenate(high, axis=0)
    return lax.ppermute(low, axis, ring(axis, 1)), lax.ppermute(high, axis, ring(axis, -1))


def exchange(x, axis):
    return lax.all_to_all(x, axis, split_axis=0, concat_axis=0, tiled=True)


def on_device(
    query_vectors,
    attend_lookup_vectors,
    attend_content_vectors,
    forget_speed_dependent,
    amend_speed_dependent,
    result_switch_preactivation,
    feature_forget_baseline,
    amend_speed_baseline,
    sudden_forget_extra,
    group_scaling_factor,
    result_mapping_matrix,
    specialist_tokens_activations,
    specialist_scaling_factor,
    selected_specialists,
    selection_mixing_factors,
    dispatched_switch_matrix,
    dispatched_raising_matrix,
    dispatched_lowering_matrix,
    common_switch_matrix,
    common_raising_matrix,
    common_lowering_matrix,
):
    tok_rows, top_count = selected_specialists.shape
    model = specialist_tokens_activations.shape[1]
    experts = lax.axis_size("ep")
    tp_size = lax.axis_size("tp")
    cap = 3 * tok_rows * top_count // (2 * experts)
    slot_rows = cap * 4 // 3
    main = model * 3 // 4
    third = model // 4
    total = experts * slot_rows

    ff = dispatched_switch_matrix.shape[2]
    me = lax.axis_index("tp").astype(jnp.int32).reshape(1)
    place = lax.axis_index("ep").astype(jnp.int32).reshape(1)

    gate_own, up_own, down_own = (
        dispatched_switch_matrix[0],
        dispatched_raising_matrix[0],
        dispatched_lowering_matrix[0],
    )
    gate_near = from_near(gate_own, "tp")
    up_near = from_near(up_own, "tp")
    down_near = from_near(down_own, "tp")
    both_far = from_far((gate_near, up_near), "tp")
    down_far = from_far((down_near,), "tp")

    normed, outgoing, positions = pl.pallas_call(
        bind(dispatch_kernel, slot_rows, cap),
        out_shape=[
            jax.ShapeDtypeStruct((tok_rows, model), BF16),
            jax.ShapeDtypeStruct((total, main), BF16),
            jax.ShapeDtypeStruct((tok_rows, top_count), jnp.int32),
        ],
        compiler_params=params(),
        name="dispatch",
    )(specialist_tokens_activations, specialist_scaling_factor.reshape(1, -1), selected_specialists.T)

    normed_near = from_near(normed, "tp")
    normed_far = from_far((normed_near,), "tp")

    received = exchange(outgoing.reshape(experts, slot_rows, main), "ep").reshape(total, main)

    out_local, q2, own_state = run_mixer_local(
        query_vectors,
        attend_lookup_vectors,
        attend_content_vectors,
        forget_speed_dependent,
        amend_speed_dependent,
        sudden_forget_extra,
        feature_forget_baseline,
        amend_speed_baseline,
    )
    all_states = lax.all_gather(own_state, "ep")
    starts = run_chain(place, all_states)

    in_vmem = pl.BlockSpec(memory_space=pltpu.MemorySpace.VMEM)
    kept = experts * cap
    rows, part = pl.pallas_call(
        bind(near_kernel, slot_rows, cap),
        in_specs=[in_vmem] * 10,
        out_specs=[in_vmem] * 2,
        out_shape=[
            jax.ShapeDtypeStruct((kept, model), BF16),
            jax.ShapeDtypeStruct((kept, model), F32),
        ],
        scratch_shapes=[pltpu.VMEM((kept, 3 * ff), BF16)],
        compiler_params=params(SMALL_LIMIT),
        name="near",
    )(received, gate_own, *gate_near, up_own, *up_near, down_own, *down_near)
    returning = pl.pallas_call(
        bind(far_kernel, slot_rows, cap),
        in_specs=[in_vmem] * 6,
        out_shape=jax.ShapeDtypeStruct((total, main), BF16),
        scratch_shapes=[pltpu.VMEM((kept, ff), BF16), pltpu.VMEM((kept, third), BF16)],
        compiler_params=params(SMALL_LIMIT),
        name="far",
    )(rows, part, *both_far, *down_far)
    expert_out = exchange(returning.reshape(experts, slot_rows, main), "ep").reshape(total, main)

    shared_part = pl.pallas_call(
        shared_kernel,
        out_shape=[jax.ShapeDtypeStruct((tok_rows, model), BF16)] * tp_size,
        compiler_params=params(),
        name="shared",
    )(
        normed,
        normed_near[1],
        *normed_far,
        normed_near[0],
        common_switch_matrix,
        common_raising_matrix,
        common_lowering_matrix,
    )
    shared_blocks = turn_exchange(shared_part, "tp")

    mixed_part = run_mixer_final(
        me,
        out_local,
        q2,
        starts,
        result_switch_preactivation,
        group_scaling_factor,
        result_mapping_matrix,
        tp_size,
    )
    mixed_blocks = turn_exchange(mixed_part, "tp")
    mixed_sum = mixed_blocks[0].astype(F32)
    for block in mixed_blocks[1:]:
        mixed_sum = mixed_sum + block.astype(F32)
    attend_result_matrix = mixed_sum.astype(BF16)
    weights, base = pl.pallas_call(
        bind(prepare_kernel, slot_rows, cap),
        out_shape=[
            jax.ShapeDtypeStruct((6 * tok_rows, total), BF16),
            jax.ShapeDtypeStruct((tok_rows, model), F32),
        ],
        compiler_params=params(),
        name="prepare",
    )(positions, selection_mixing_factors, *shared_blocks)
    moe_out = pl.pallas_call(
        combine_kernel,
        in_specs=[in_vmem] * 3,
        out_shape=jax.ShapeDtypeStruct((tok_rows, model), BF16),
        compiler_params=params(),
        name="combine",
    )(expert_out, weights, base)
    return (attend_result_matrix, moe_out)


def solution(mesh):
    by_rows = P(("grp", "ep"), "tp")
    by_device = P(("grp", "ep", "tp"), None)
    placed = (
        by_rows,
        by_rows,
        by_rows,
        by_rows,
        by_rows,
        by_rows,
        P("tp"),
        P("tp"),
        by_rows,
        P("tp"),
        P("tp", None),
        by_device,
        P(),
        by_device,
        by_device,
        P("ep", None, "tp"),
        P("ep", None, "tp"),
        P("ep", "tp", None),
        P(None, "tp"),
        P(None, "tp"),
        P("tp", None),
    )
    return jax.shard_map(
        on_device, mesh=mesh, in_specs=placed, out_specs=(by_device, by_device), check_vma=False
    )
```
